32 devices in a mesh: rep: 2 (over x), fs: 8 (over z, y), tp: 2 (over core).
Axes of the slice: x: 2, y: 2, z: 4, core: 2. Of those that a mesh axis runs over, the one named last changes fastest.
Arguments:
- inputs: bfloat16 [8192, 2048], P(('rep', 'fs')), may hold values from -6 to 6
- gain: float32 [2048], replicated, may hold values from 0.1 to 1.9
- gate_weight: bfloat16 [2048, 3072], P('fs', 'tp'), may hold values from -0.125 to 0.125
- up_weight: bfloat16 [2048, 3072], P('fs', 'tp'), may hold values from -0.125 to 0.125
- down_weight: bfloat16 [2048, 3072], P('fs', 'tp'), may hold values from -0.109375 to 0.109375
- cotangent: bfloat16 [8192, 2048], P(('rep', 'fs')), may hold values from -6 to 6
Outputs:
- input_gradient: bfloat16 [8192, 2048], P(('rep', 'fs'))
- gain_gradient: float32 [2048], replicated
- d_down: float32 [2048, 3072], P('fs', 'tp')
The draws below stay inside these ranges and needn't reach their ends.
All inputs are finite; a program needn't handle non-finite values.
Results may differ from the reference program's by a relative error of at most 0.014.
Values may be sent and summed in bfloat16 or wider, within the bound.
A program may use at most 128 MiB of HBM per device.

```python
import jax
import jax.numpy as jnp
from jax import lax

D = 2048
FF = 3072
TOKENS = 8192
N_TP = 2


def with_spikes(result, stream_key, source, target, blocks, factor):
    owner, partner = [(jnp.arange(result.shape[dim]) // (result.shape[dim] // blocks)).reshape([-1 if axis == dim else 1 for axis in range(result.ndim)]) for dim in (source, target)]
    chosen = jax.random.permutation(stream_key, blocks)[partner]
    strong = (owner == chosen) | (owner == (partner + blocks // 2) % blocks)
    return jnp.where(strong, factor * result, result)


def shard_levels(rng, dims, split, least, high):
    def one(dim, parts):
        steps = jax.random.uniform(jax.random.fold_in(jax.random.fold_in(rng, 6), dim), (parts,), jnp.float32, least / len(split), high / len(split))
        return jnp.repeat(jnp.exp(steps), dims[dim] // parts).reshape((-1,) + (1,) * (len(dims) - dim - 1))

    factor_of = one(*split[0])
    for cut in split[1:]:
        factor_of = factor_of * one(*cut)
    return factor_of


def gaussian(rng, shape, width, bound, split=(), dtype=jnp.bfloat16):
    drawn = width * jax.random.normal(rng, shape, jnp.float32)
    if split:
        drawn = drawn * shard_levels(rng, shape, split, -0.22, 0.18)
    return jnp.clip(drawn, -bound, bound).astype(dtype)


def bell_draw_with(stream_key, extent, scale, reach, cuts, heavy, held_as=jnp.bfloat16):
    array = scale * jax.random.normal(stream_key, extent, jnp.float32)
    if cuts:
        array = array * shard_levels(stream_key, extent, cuts, -0.22, 0.18)
    return jnp.clip(with_spikes(array, jax.random.fold_in(stream_key, 3), *heavy), -reach, reach).astype(held_as)


def setup_inputs(seed: int = 0) -> dict:
    key_of = jax.random.split(jax.random.key(seed), 7)
    inputs = gaussian(key_of[0], (TOKENS, D), 1.0, 6.0, ((0, 16),))
    gain = jnp.clip(1.0 + 0.18 * jax.random.normal(key_of[1], (D,), jnp.float32), 0.1, 1.9)
    gate_weight = gaussian(key_of[2], (D, FF), D ** -0.5, 0.125, ((0, 8), (1, 2)))
    up_weight = gaussian(key_of[3], (D, FF), D ** -0.5, 0.125, ((0, 8), (1, 2)))
    down_weight = gaussian(key_of[4], (D, FF), FF ** -0.5, 0.109375, ((0, 8), (1, 2)))
    cotangent = bell_draw_with(key_of[5], (TOKENS, D), 1.0, 6.0, ((0, 16),), (0, 1, 16, 2.0))
    return {"inputs": inputs, "gain": gain, "gate_weight": gate_weight, "up_weight": up_weight, "down_weight": down_weight, "cotangent": cotangent}


EPS = 1e-06

def reference(inputs, gain, gate_weight, up_weight, down_weight, cotangent):
    single_precision = inputs.astype(jnp.float32)
    reciprocal_root_mean = lax.rsqrt(lax.optimization_barrier(jnp.mean(single_precision * single_precision, axis=-1, keepdims=True)) + EPS)
    unit_input = single_precision * reciprocal_root_mean
    normalized_input = (unit_input * gain).astype(jnp.bfloat16)
    gate = jnp.dot(normalized_input, gate_weight, preferred_element_type=jnp.float32)
    up_proj = jnp.dot(normalized_input, up_weight, preferred_element_type=jnp.float32)
    gate_sig = jax.nn.sigmoid(gate)
    active = gate * gate_sig
    hidden = (active * up_proj).astype(jnp.bfloat16)
    d_hidden = 0.5 * lax.dot_general(cotangent, down_weight, (((1,), (0,)), ((), ())), preferred_element_type=jnp.float32)
    d_down = 0.5 * lax.dot_general(cotangent, hidden, (((0,), (0,)), ((), ())), preferred_element_type=jnp.float32)
    d_gate = (d_hidden * up_proj * gate_sig * (1.0 + gate * (1.0 - gate_sig))).astype(jnp.bfloat16)
    d_up = (d_hidden * active).astype(jnp.bfloat16)
    unit_width = FF // N_TP
    normalized_gradient = jnp.zeros(single_precision.shape, jnp.float32)
    for column_block in range(N_TP):
        first = column_block * unit_width
        partial_value = lax.dot_general(d_gate[:, first:first + unit_width], gate_weight[:, first:first + unit_width], (((1,), (1,)), ((), ())), preferred_element_type=jnp.float32)
        partial_value = partial_value + lax.dot_general(d_up[:, first:first + unit_width], up_weight[:, first:first + unit_width], (((1,), (1,)), ((), ())), preferred_element_type=jnp.float32)
        rounded = lax.optimization_barrier(partial_value.astype(jnp.bfloat16))
        normalized_gradient = normalized_gradient + rounded.astype(jnp.float32)
    summed_rounded = lax.optimization_barrier(normalized_gradient.astype(jnp.bfloat16))
    normalized_gradient = summed_rounded.astype(jnp.float32)
    gain_gradient = lax.optimization_barrier(jnp.sum(normalized_gradient * unit_input, axis=0))
    gain_scaled = gain * normalized_gradient
    mean_correction = lax.optimization_barrier(jnp.mean(gain_scaled * unit_input, axis=-1, keepdims=True))
    input_gradient = (cotangent.astype(jnp.float32) + reciprocal_root_mean * (gain_scaled - unit_input * mean_correction)).astype(jnp.bfloat16)
    return (input_gradient, gain_gradient, d_down)
```

```python
import functools

import jax
import jax.numpy as jnp
from jax import lax
from jax.experimental import pallas as pl
from jax.experimental.pallas import tpu as pltpu
from jax.sharding import PartitionSpec as P

EPS = 1e-06
F32, BF16 = jnp.float32, jnp.bfloat16
MESH_ID = pl.DeviceIdType.MESH
N_Y, N_Z = 2, 4
CHUNKS = 3
TOKEN_PARTS = 4
BACK_PARTS = 4


class Slots:
    def __init__(self):
        self.slots = {}

    def __call__(self, *key):
        return self.slots.setdefault(key, len(self.slots))


def all_slots():
    slots = Slots()
    for u in range(CHUNKS):
        for w in range(3):
            slots("yw", u, w)
            for k in range(1, N_Z):
                slots("up", u, w, k)
                slots("dn", u, w, k)
                slots("xw", u, w, k)
        for k in range(N_Z):
            slots("rx", u, k)
            slots("rz", u, k)
        slots("ry", u)
        slots("fx", u, 0)
        slots("fx", u, 1)
    for a in range(2):
        for i in range(TOKEN_PARTS):
            slots("yt", a, i)
            slots("ct", a, i)
    for h in range(2):
        slots("cd", h)
    for i in range(BACK_PARTS):
        slots("yd", i)
        slots("ig", i)
    for i in range(5):
        slots("gg", i)
    return slots


def fused_kernel(
    x, gain, gate_w, up_w, down_w, ct,
    ig, gg, dd,
    wgu, wd, xall, ctall, xn, inv, hid, dgu, dn, dd32, ddb, rx, zs, rz, fin, ry, fx,
    sd, rd, sy, yd, igv, gsend, grecv, ddv, gvec,
    send, recv, own,
):
    slots = all_slots()
    rep, fs, tp = lax.axis_index("rep"), lax.axis_index("fs"), lax.axis_index("tp")
    z, y = fs // N_Y, fs % N_Y
    b = (rep + y) % 2
    rows, width = x.shape
    wrows, cols = gate_w.shape
    units = cols // N_Y
    uc = units // CHUNKS
    half = rows // 2
    to_x, to_c = {"rep": 1 - rep}, {"tp": 1 - tp}
    to_y = {"fs": z * N_Y + 1 - y}
    to_up, to_dn = {"fs": fs + N_Y}, {"fs": fs - N_Y}
    z1 = z + 1 - 2 * (z % 2)
    z2 = (z + 2) % N_Z
    z3 = N_Z - 1 - z
    to_z = {1: {"fs": z1 * N_Y + y}, 2: {"fs": z2 * N_Y + y}, 3: {"fs": z3 * N_Y + y}}
    z_of = {1: z1, 2: z2, 3: z3}

    barrier = pltpu.get_barrier_semaphore()
    for target in (to_x, to_c, to_y, to_z[1], to_z[2], to_z[3]):
        pl.semaphore_signal(barrier, inc=1, device_id=target, device_id_type=MESH_ID)
    pl.semaphore_wait(barrier, 6)

    pending = []

    def remote(key, src, dst, target):
        i = slots(*key)
        return pltpu.make_async_remote_copy(
            src_ref=src, dst_ref=dst, send_sem=send.at[i], recv_sem=recv.at[i],
            device_id=target, device_id_type=MESH_ID,
        )

    def start(key, src, dst, target, cond=None):
        remote(key, src, dst, target).start()
        pending.append((key, src, cond))

    def wait(key, like):
        remote(key, like, like, to_x).wait_recv()

    def region(u, w, owner):
        r = pl.ds(pl.multiple_of(owner * wrows, wrows), wrows)
        if w == 2:
            return wd.at[u, r]
        return wgu.at[u, r, pl.ds(w * uc, uc)]

    weights = (gate_w, up_w, down_w)

    def part(w, who, u):
        return weights[w].at[:, pl.ds(pl.multiple_of(who * units + u * uc, uc), uc)]

    def y_weights(u, w):
        start(("yw", u, w), part(w, 1 - y, u), region(u, w, fs), to_y)

    own_tokens = pl.multiple_of(y * rows, rows)
    other_tokens = pl.multiple_of((1 - y) * rows, rows)
    tpart = half // TOKEN_PARTS

    def y_tokens(a, i):
        full = (xall, ctall)[a]
        r = pl.ds(pl.multiple_of(own_tokens + tp * half + i * tpart, tpart), tpart)
        start(("yt", a, i), full.at[r], full.at[r], to_y)

    def core_tokens(a, i):
        full = (xall, ctall)[a]
        r = pl.ds(pl.multiple_of(other_tokens + tp * half + i * tpart, tpart), tpart)
        wait(("yt", a, i), full.at[r])
        start(("ct", a, i), full.at[r], full.at[r], to_c)

    def core_wait(a, i):
        full = (xall, ctall)[a]
        r = pl.ds(pl.multiple_of(other_tokens + tp * half + i * tpart, tpart), tpart)
        wait(("ct", a, i), full.at[r])

    pieces = [(u, w) for u in range(CHUNKS) for w in range(3)]
    for u, w in pieces[:3]:
        y_weights(u, w)
    kept = []
    for a, (source, full) in enumerate(((x, xall), (ct, ctall))):
        kept.append(
            pltpu.make_async_copy(source, full.at[pl.ds(own_tokens, rows)], own.at[a])
        )
    for n, (u, w) in enumerate(pieces):
        kept.append(pltpu.make_async_copy(part(w, y, u), region(u, w, fs), own.at[2 + n]))
    for copy in kept[2:5] + kept[:2] + kept[5:]:
        copy.start()

    def own_send(n):
        u, w = pieces[n]
        kept[2 + n].wait()

        @pl.when(rep == 1)
        def _():
            wait(("yw", u, w), region(u, w, fs))

        src = region(u, w, z * N_Y + b)

        @pl.when(z < N_Z - 1)
        def _():
            start(("up", u, w, 1), src, src, to_up, lambda: z < N_Z - 1)

        @pl.when(z > 0)
        def _():
            start(("dn", u, w, 1), src, src, to_dn, lambda: z > 0)

    def arrive(n, d):
        u, w = pieces[n]

        @pl.when(z - d >= 0)
        def _():
            src = region(u, w, (z - d) * N_Y + b)
            wait(("up", u, w, d), src)
            if d < N_Z - 1:

                @pl.when(z < N_Z - 1)
                def _():
                    start(("up", u, w, d + 1), src, src, to_up, lambda: (z - d >= 0) & (z < N_Z - 1))

            remote(("xw", u, w, N_Z - d), src, src, to_x).start()

        @pl.when(z + d <= N_Z - 1)
        def _():
            src = region(u, w, (z + d) * N_Y + b)
            wait(("dn", u, w, d), src)
            if d < N_Z - 1:

                @pl.when(z > 0)
                def _():
                    start(("dn", u, w, d + 1), src, src, to_dn, lambda: (z + d <= N_Z - 1) & (z > 0))

            remote(("xw", u, w, d), src, src, to_x).start()

    def chunk_ready(u):
        for w in range(3):
            like = region(u, w, fs)

            @pl.when(rep == 0)
            def _():
                wait(("yw", u, w), like)

            for k in range(1, N_Z):
                wait(("xw", u, w, k), like)

    for n in range(3):
        own_send(n)
    kept[0].wait()
    kept[1].wait()

    gain_row = gain[...]
    norm_rows = 64

    def normalize(first):
        def body(i, _):
            r = pl.ds(pl.multiple_of(first + i * norm_rows, norm_rows), norm_rows)
            single = xall[r, :].astype(F32)
            scale = lax.rsqrt(jnp.mean(single * single, axis=-1, keepdims=True) + EPS)
            inv[r, :] = scale
            xn[r, :] = (single * scale * gain_row).astype(BF16)
            return 0

        lax.fori_loop(0, rows // norm_rows, body, 0)

    def forward(u, first):
        r = pl.ds(first, rows)
        both = jnp.dot(xn[r, :], wgu[u], preferred_element_type=F32)
        gate, up = both[:, :uc], both[:, uc:]
        sig = jax.nn.sigmoid(gate)
        active = gate * sig
        hid[u, r, :] = (active * up).astype(BF16)
        d_hidden = 0.5 * jnp.dot(ctall[r, :], wd[u], preferred_element_type=F32)
        dgu[u, r, :uc] = (d_hidden * up * sig * (1.0 + gate * (1.0 - sig))).astype(BF16)
        dgu[u, r, uc:] = (d_hidden * active).astype(BF16)

    over_rows = (((0,), (0,)), ((), ()))
    over_cols = (((1,), (1,)), ((), ()))

    def down_terms(u):
        def body(zd, _):
            r = pl.ds(pl.multiple_of(zd * 2 * wrows, 2 * wrows), 2 * wrows)
            value = 0.5 * lax.dot_general(
                ctall[:, r], hid[u], over_rows, preferred_element_type=F32
            )
            dd32[u, zd] = value.reshape(2, 2, wrows // 2, uc)
            ddb[u, zd] = dd32[u, zd, :, 1 - rep].astype(BF16)
            return 0

        lax.fori_loop(0, N_Z, body, 0)
        for k in (3, 2, 1, 0):
            zd = z if k == 0 else z_of[k]
            start(("rx", u, k), ddb.at[u, zd], rx.at[u, zd], to_x)

    def down_along_z(u, k):
        zd = z if k == 0 else z_of[k]
        wait(("rx", u, k), rx.at[u, zd])
        total = dd32[u, zd, :, rep] + rx[u, zd].astype(F32)
        if k == 0:
            fin[u] = total
        else:
            zs[u, k] = total.astype(BF16)
            start(("rz", u, k), zs.at[u, k], rz.at[u, k], to_z[k])

    def put(u, side, who, value):
        r = pl.ds(pl.multiple_of(side * (wrows // 2), wrows // 2), wrows // 2)
        c = pl.ds(pl.multiple_of(who * units + u * uc, uc), uc)
        ddv[r, c] = value

    fb = zs

    def down_final(u):
        total = fin[u]
        for k in range(1, N_Z):
            wait(("rz", u, k), rz.at[u, k])
            total = total + rz[u, k].astype(F32)
        fin[u] = total
        fb[u, 0] = total.astype(BF16)
        start(("ry", u), fb.at[u, 0, 1 - y], ry.at[u], to_y)
        start(("fx", u, 0), fb.at[u, 0, y], fx.at[u, 0], to_x)
        put(u, rep, y, fb[u, 0, y])

    def down_y(u):
        wait(("ry", u), ry.at[u])
        start(("fx", u, 1), ry.at[u], fx.at[u, 1], to_x)
        put(u, rep, 1 - y, ry[u])

    def down_x(u):
        wait(("fx", u, 0), fx.at[u, 0])
        put(u, 1 - rep, y, fx[u, 0])
        wait(("fx", u, 1), fx.at[u, 1])
        put(u, 1 - rep, 1 - y, fx[u, 1])

    n_cols = 512

    def back(first):
        def body(j, _):
            c = pl.ds(pl.multiple_of(j * n_cols, n_cols), n_cols)
            total = None
            for u in range(CHUNKS):
                term = lax.dot_general(
                    dgu[u, pl.ds(first, rows), :], wgu[u, c, :], over_cols,
                    preferred_element_type=F32,
                )
                total = term if total is None else total + term
            dn[pl.ds(first, rows), c] = total
            return 0

        lax.fori_loop(0, width // n_cols, body, 0)

    def back_to_core(h, first):
        r = pl.ds(pl.multiple_of(first + (1 - tp) * half, half), half)
        sd[h] = dn[r, :].astype(BF16)
        start(("cd", h), sd.at[h], rd.at[h], to_c)

    bpart = half // BACK_PARTS

    def back_to_y():
        wait(("cd", 0), rd.at[0])
        for i in range(BACK_PARTS):
            r = pl.ds(pl.multiple_of(other_tokens + tp * half + i * bpart, bpart), bpart)
            q = pl.ds(i * bpart, bpart)
            mine = dn[r, :].astype(BF16).astype(F32)
            sy[q, :] = (mine + rd[0, q, :].astype(F32)).astype(BF16)
            start(("yd", i), sy.at[q], yd.at[q], to_y)

    def gain_terms(first):
        def body(i, acc):
            r = pl.ds(pl.multiple_of(first + i * norm_rows, norm_rows), norm_rows)
            terms = dn[r, :] * (xall[r, :].astype(F32) * inv[r, :])
            return acc + jnp.sum(terms.reshape(norm_rows // 8, 8, width), axis=0)

        return lax.fori_loop(0, rows // norm_rows, body, jnp.zeros((8, width), F32))

    gain_targets = (to_c, to_y, to_x, to_z[1], to_z[2])

    def gain_send(i):
        gsend[i] = gvec[...]
        start(("gg", i), gsend.at[i], grecv.at[i], gain_targets[i])

    def gain_recv(i):
        wait(("gg", i), grecv.at[i])
        gvec[...] = gvec[...] + grecv[i]

    out_row = pl.multiple_of(tp * half, half)

    def back_final(i):
        q = pl.ds(i * bpart, bpart)
        wait(("yd", i), yd.at[q])
        r = pl.ds(pl.multiple_of(own_tokens + tp * half + i * bpart, bpart), bpart)
        mine = dn[r, :].astype(BF16).astype(F32) + rd[1, q, :].astype(F32)
        mine = mine.astype(BF16).astype(F32) + yd[q, :].astype(F32)
        mine = mine.astype(BF16).astype(F32)
        scale = inv[r, :]
        unit = xall[r, :].astype(F32) * scale
        scaled = gain_row * mine
        mean = jnp.mean(scaled * unit, axis=-1, keepdims=True)
        o = pl.ds(pl.multiple_of(out_row + i * bpart, bpart), bpart)
        igv[o, :] = (ctall[r, :].astype(F32) + scale * (scaled - unit * mean)).astype(BF16)
        start(("ig", i), igv.at[o], igv.at[o], to_c)

    normalize(own_tokens)
    token_order = [(a, i) for a in range(2) for i in range(TOKEN_PARTS)]
    last = len(pieces)
    for t in range(last + 2):
        if t + 3 < last:
            y_weights(*pieces[t + 3])
        if t < len(token_order):
            y_tokens(*token_order[t])
        if t + 2 < last and t + 2 >= 3:
            own_send(t + 2)
        for d in range(1, N_Z):
            if 0 <= t + 1 - d < last:
                arrive(t + 1 - d, d)
        if 3 <= t < len(token_order) + 3:
            core_tokens(*token_order[t - 3])
    for a, i in token_order:
        core_wait(a, i)
    normalize(other_tokens)
    for u in range(CHUNKS):
        chunk_ready(u)
        forward(u, own_tokens)
        forward(u, other_tokens)
        down_terms(u)
    back(other_tokens)
    back_to_core(0, other_tokens)
    for k in (3, 2, 1, 0):
        down_along_z(0, k)
    back_to_y()
    back(own_tokens)
    back_to_core(1, own_tokens)
    acc = gain_terms(own_tokens) + gain_terms(other_tokens)
    gvec[...] = jnp.sum(acc, axis=0, keepdims=True)
    gain_send(0)
    for k in (3, 2, 1, 0):
        down_along_z(1, k)
    gain_recv(0)
    gain_send(1)
    down_final(0)
    gain_recv(1)
    gain_send(2)
    wait(("cd", 1), rd.at[1])
    for k in (3, 2, 1, 0):
        down_along_z(2, k)
    gain_recv(2)
    gain_send(3)
    down_y(0)
    down_final(1)
    gain_recv(3)
    gain_send(4)
    down_x(0)
    down_y(1)
    gain_recv(4)
    back_final(0)
    back_final(1)
    down_x(1)
    down_final(2)
    back_final(2)
    down_y(2)
    back_final(3)
    down_x(2)
    for i in range(BACK_PARTS):
        o = pl.ds(pl.multiple_of(i * bpart, bpart), bpart)
        wait(("ig", i), igv.at[o])
    gg_copy = pltpu.make_async_copy(gvec, gg, own.at[0])
    ig_copy = pltpu.make_async_copy(igv, ig, own.at[1])
    dd_copy = pltpu.make_async_copy(ddv, dd, own.at[2])
    for copy in (ig_copy, dd_copy, gg_copy):
        copy.start()
    for u, w in pieces:
        for k in range(1, N_Z):
            like = region(u, w, fs)
            remote(("xw", u, w, k), like, like, to_x).wait_send()
    for key, src, cond in pending:
        if cond is None:
            remote(key, src, src, to_x).wait_send()
        else:

            @pl.when(cond())
            def _():
                like = region(key[1], key[2], fs)
                remote(key, like, like, to_x).wait_send()

    for copy in (ig_copy, dd_copy, gg_copy):
        copy.wait()


def fused(x, gain, gate_w, up_w, down_w, ct):
    rows, width = x.shape
    wrows, cols = gate_w.shape
    units = cols // N_Y
    uc = units // CHUNKS
    half = rows // 2
    n = len(all_slots().slots)
    vm = pltpu.VMEM
    anywhere = pl.BlockSpec(memory_space=pl.ANY)
    tile = (2, wrows // 2, uc)
    ig, gg, dd = pl.pallas_call(
        fused_kernel,
        out_shape=[
            jax.ShapeDtypeStruct((rows, width), BF16),
            jax.ShapeDtypeStruct((1, width), F32),
            jax.ShapeDtypeStruct((wrows, cols), BF16),
        ],
        in_specs=[anywhere, pl.BlockSpec(memory_space=vm)] + [anywhere] * 4,
        out_specs=[anywhere] * 3,
        scratch_shapes=[
            vm((CHUNKS, width, 2 * uc), BF16),
            vm((CHUNKS, width, uc), BF16),
            vm((2 * rows, width), BF16),
            vm((2 * rows, width), BF16),
            vm((2 * rows, width), BF16),
            vm((2 * rows, 1), F32),
            vm((CHUNKS, 2 * rows, uc), BF16),
            vm((CHUNKS, 2 * rows, 2 * uc), BF16),
            vm((2 * rows, width), F32),
            vm((CHUNKS, N_Z, 2) + tile, F32),
            vm((CHUNKS, N_Z) + tile, BF16),
            vm((CHUNKS, N_Z) + tile, BF16),
            vm((CHUNKS, N_Z) + tile, BF16),
            vm((CHUNKS, N_Z) + tile, BF16),
            vm((CHUNKS,) + tile, F32),
            vm((CHUNKS,) + tile[1:], BF16),
            vm((CHUNKS,) + tile, BF16),
            vm((2, half, width), BF16),
            vm((2, half, width), BF16),
            vm((half, width), BF16),
            vm((half, width), BF16),
            vm((rows, width), BF16),
            vm((5, 1, width), F32),
            vm((5, 1, width), F32),
            vm((wrows, cols), BF16),
            vm((1, width), F32),
            pltpu.SemaphoreType.DMA((n,)),
            pltpu.SemaphoreType.DMA((n,)),
            pltpu.SemaphoreType.DMA((2 + 3 * CHUNKS,)),
        ],
        compiler_params=pltpu.CompilerParams(
            collective_id=0, has_side_effects=True, vmem_limit_bytes=67043328
        ),
        name="fused",
    )(x, gain.reshape(1, width), gate_w, up_w, down_w, ct)
    return ig, gg.reshape(width), dd.astype(F32)


def shift(value, axis, step):
    size = lax.axis_size(axis)
    return lax.ppermute(value, axis, [(i, (i + step) % size) for i in range(size)])


def swap(value, axis, bit):
    return lax.ppermute(value, axis, [(i, i ^ bit) for i in range(lax.axis_size(axis))])


def summed_everywhere(value):
    for axis in ("rep", "fs", "tp"):
        size = lax.axis_size(axis)
        if size & (size - 1):
            value = lax.psum(value, axis)
            continue
        bit = 1
        while bit < size:
            value = value + swap(value, axis, bit)
            bit *= 2
    return value


def local(inputs, gain, gate_weight, up_weight, down_weight, cotangent):
    n_rep, n_tp = lax.axis_size("rep"), lax.axis_size("tp")
    if (n_rep, lax.axis_size("fs"), n_tp) == (2, N_Y * N_Z, 2):
        return fused(inputs, gain, gate_weight, up_weight, down_weight, cotangent)
    rep, tp = lax.axis_index("rep"), lax.axis_index("tp")
    rows, width = inputs.shape
    block = rows // n_tp
    units = gate_weight.shape[1] // n_rep

    def own_units(weight):
        return lax.dynamic_slice_in_dim(weight, rep * units, units, axis=1)

    def own_block(value, step):
        return lax.dynamic_slice_in_dim(value, (tp + step) % n_tp * block, block, axis=0)

    def gathered_tokens(value):
        parts = [own_block(value, s) for s in range(n_tp)]
        for j in range(1, n_rep):
            first = shift(own_block(value, 0), "rep", -j)
            parts += [first] + [shift(first, "tp", -s) for s in range(1, n_tp)]
        return jnp.concatenate(parts, axis=0)

    both_own = jnp.concatenate([own_units(gate_weight), own_units(up_weight)], axis=1)
    both_full = lax.all_gather(both_own, "fs", axis=0, tiled=True)
    down_full = lax.all_gather(own_units(down_weight), "fs", axis=0, tiled=True)
    tokens = gathered_tokens(inputs)
    cots = gathered_tokens(cotangent)

    def normed(value):
        single = value.astype(jnp.float32)
        inv = lax.rsqrt(jnp.mean(single * single, axis=-1, keepdims=True) + EPS)
        return single * inv, inv

    normalized_input = (normed(tokens)[0] * gain).astype(jnp.bfloat16)
    contract_cols = (((1,), (1,)), ((), ()))
    contract_rows = (((0,), (0,)), ((), ()))
    both = jnp.dot(normalized_input, both_full, preferred_element_type=jnp.float32)
    gate, up_proj = both[:, :units], both[:, units:]
    gate_sig = jax.nn.sigmoid(gate)
    active = gate * gate_sig
    hidden = (active * up_proj).astype(jnp.bfloat16)
    d_down_terms = (
        0.5 * lax.dot_general(cots, hidden, contract_rows, preferred_element_type=jnp.float32)
    ).astype(jnp.bfloat16)
    d_down_terms, cots = lax.optimization_barrier((d_down_terms, cots))
    summed = lax.psum_scatter(d_down_terms, "fs", scatter_dimension=0, tiled=True)
    d_hidden = 0.5 * jnp.dot(cots, down_full, preferred_element_type=jnp.float32)
    d_gate = (d_hidden * up_proj * gate_sig * (1.0 + gate * (1.0 - gate_sig))).astype(jnp.bfloat16)
    d_up = (d_hidden * active).astype(jnp.bfloat16)
    partial_value = (
        lax.dot_general(
            jnp.concatenate([d_gate, d_up], axis=1),
            both_full,
            contract_cols,
            preferred_element_type=jnp.float32,
        )
    ).astype(jnp.bfloat16).reshape(n_rep, n_tp, block, width)

    def tp_terms(step):
        return partial_value[:, step]

    over_tp = tp_terms(0).astype(jnp.float32)
    for s in range(1, n_tp):
        over_tp = over_tp + shift(tp_terms(s), "tp", s).astype(jnp.float32)
    over_tp = over_tp.astype(jnp.bfloat16)
    total = over_tp[0].astype(jnp.float32)
    for j in range(1, n_rep):
        total = total + shift(over_tp[j], "rep", j).astype(jnp.float32)
    normalized_gradient = total.astype(jnp.bfloat16).astype(jnp.float32)
    unit_input, inv = normed(own_block(inputs, 0))
    gain_gradient = summed_everywhere(jnp.sum(normalized_gradient * unit_input, axis=0))
    gain_scaled = gain * normalized_gradient
    mean_correction = jnp.mean(gain_scaled * unit_input, axis=-1, keepdims=True)
    block_gradient = (
        own_block(cotangent, 0).astype(jnp.float32)
        + inv * (gain_scaled - unit_input * mean_correction)
    ).astype(jnp.bfloat16)
    input_gradient = jnp.zeros((rows, width), jnp.bfloat16)
    for s in range(n_tp):
        piece = block_gradient if s == 0 else shift(block_gradient, "tp", -s)
        input_gradient = lax.dynamic_update_slice_in_dim(
            input_gradient, piece, (tp + s) % n_tp * block, axis=0
        )
    d_down = jnp.zeros((summed.shape[0], units * n_rep), jnp.float32)
    for j in range(n_rep):
        piece = summed if j == 0 else shift(summed, "rep", -j)
        d_down = lax.dynamic_update_slice_in_dim(
            d_down, piece.astype(jnp.float32), (rep + j) % n_rep * units, axis=1
        )
    return (input_gradient, gain_gradient, d_down)


def solution(mesh):
    placed = (
        P(("rep", "fs"), None),
        P(),
        P("fs", "tp"),
        P("fs", "tp"),
        P("fs", "tp"),
        P(("rep", "fs"), None),
    )
    return jax.shard_map(
        local,
        mesh=mesh,
        in_specs=placed,
        out_specs=(P(("rep", "fs"), None), P(), P("fs", "tp")),
        check_vma=False,
    )
```

```python
import jax
import jax.numpy as jnp
from jax import lax
from jax.experimental import pallas as pl
from jax.experimental.pallas import tpu as pltpu
from jax.sharding import PartitionSpec as P

EPS = 1e-06
F32, BF16 = jnp.float32, jnp.bfloat16
MESH_ID = pl.DeviceIdType.MESH
N_Y, N_Z = 2, 4
GATHER = ("yw", "yt", "ct", "up", "dn", "xw", "zh", "cd")
CHUNKS = 3
TOKEN_PARTS = 4
BACK_PARTS = 8


ORDER = ((0, 2, 1, 4, 3, 5, 6, 7, 8), (1, 3, 0, 2, 5, 4, 7, 6, 8))
Y_ORDER = tuple(
    tuple(("w", i) if isinstance(i, int) else ("t",) + i for i in order)
    for order in (
        (1, (0, 0), 3, (0, 1), 5, (0, 2), (0, 3), 0, 2, 7, (1, 0), (1, 1), (1, 2), (1, 3), 4, 6, 8),
        (0, 2, (0, 0), (0, 1), 4, (0, 2), (0, 3), 1, 6, (1, 0), 8, (1, 1), (1, 2), (1, 3), 3, 5, 7),
    )
)


class Slots:
    def __init__(self):
        self.slots = {}

    def __call__(self, *key):
        return self.slots.setdefault(key, len(self.slots))


def all_slots():
    slots = Slots()
    for u in range(CHUNKS):
        for w in range(3):
            slots("yw", u, w)
            for k in range(1, N_Z):
                slots("up", u, w, k)
                slots("dn", u, w, k)
                slots("xw", u, w, k)
        if u:
            for k in range(N_Z):
                slots("rx", u, k)
                if k:
                    slots("rz", u, k)
            slots("ry", u)
            slots("fx", u, 0)
            slots("fx", u, 1)
    for i in range(3):
        slots("zh", i)
    slots("hx")
    slots("hy")
    for a in range(2):
        for i in range(TOKEN_PARTS):
            slots("yt", a, i)
            slots("ct", a, i)
    for h in range(2):
        slots("cd", h)
    for i in range(BACK_PARTS):
        slots("yd", i)
        slots("ig", i)
    for i in range(5):
        slots("gg", i)
    return slots


def fused_kernel(
    x, gain, gate_w, up_w, down_w, ct,
    ig, gg, dd,
    wgu, wd, xall, ctall, xn, inv, hid, dgu, dn, dd32, ddb, rx, zs, rz, fin, ry, fx,
    sd, rd, sy, yd, igv, gsend, grecv, ddv, gvec, zh, zr, hx, hy,
    send, recv, own,
):
    slots = all_slots()
    rep, fs, tp = lax.axis_index("rep"), lax.axis_index("fs"), lax.axis_index("tp")
    z, y = fs // N_Y, fs % N_Y
    rows, width = x.shape
    wrows, cols = gate_w.shape
    units = cols // N_Y
    uc = units // CHUNKS
    half = rows // 2
    to_x, to_c = {"rep": 1 - rep}, {"tp": 1 - tp}
    to_y = {"fs": z * N_Y + 1 - y}
    to_up, to_dn = {"fs": fs + N_Y}, {"fs": fs - N_Y}
    z1 = z + 1 - 2 * (z % 2)
    z2 = (z + 2) % N_Z
    z3 = N_Z - 1 - z
    to_z = {1: {"fs": z1 * N_Y + y}, 2: {"fs": z2 * N_Y + y}, 3: {"fs": z3 * N_Y + y}}
    z_of = {1: z1, 2: z2, 3: z3}

    barrier = pltpu.get_barrier_semaphore()
    for target in (to_x, to_c, to_y, to_z[1], to_z[2], to_z[3]):
        pl.semaphore_signal(barrier, inc=1, device_id=target, device_id_type=MESH_ID)
    pl.semaphore_wait(barrier, 6)

    pending = {}

    def remote(key, src, dst, target):
        i = slots(*key)
        return pltpu.make_async_remote_copy(
            src_ref=src, dst_ref=dst, send_sem=send.at[i], recv_sem=recv.at[i],
            device_id=target, device_id_type=MESH_ID,
        )

    def start(key, src, dst, target, cond=None):
        remote(key, src, dst, target).start()
        pending.setdefault(key, cond)

    def wait(key, like):
        remote(key, like, like, to_x).wait_recv()

    def region(u, w, owner):
        r = pl.ds(pl.multiple_of(owner * wrows, wrows), wrows)
        if w == 2:
            return wd.at[u, r]
        return wgu.at[u, r, pl.ds(w * uc, uc)]

    weights = (gate_w, up_w, down_w)

    def part(w, who, u):
        return weights[w].at[:, pl.ds(pl.multiple_of(who * units + u * uc, uc), uc)]

    def y_weights(u, w):
        start(("yw", u, w), part(w, 1 - y, u), region(u, w, fs), to_y)

    own_tokens = pl.multiple_of(y * rows, rows)
    other_tokens = pl.multiple_of((1 - y) * rows, rows)
    tpart = half // TOKEN_PARTS

    def y_tokens(a, i):
        full = (xall, ctall)[a]
        r = pl.ds(pl.multiple_of(own_tokens + tp * half + i * tpart, tpart), tpart)
        start(("yt", a, i), full.at[r], full.at[r], to_y)

    def core_tokens(a, i):
        full = (xall, ctall)[a]
        r = pl.ds(pl.multiple_of(other_tokens + tp * half + i * tpart, tpart), tpart)
        wait(("yt", a, i), full.at[r])
        start(("ct", a, i), full.at[r], full.at[r], to_c)

    def core_wait(a, i):
        full = (xall, ctall)[a]
        r = pl.ds(pl.multiple_of(other_tokens + tp * half + i * tpart, tpart), tpart)
        wait(("ct", a, i), full.at[r])

    pieces = [(u, w) for u in range(CHUNKS) for w in range(3)]

    def local_copy(n):
        u, w = pieces[n]
        return pltpu.make_async_copy(part(w, y, u), region(u, w, fs), own.at[2 + n])

    kept = [local_copy(n) for n in range(len(pieces))]
    kept_tokens = [
        pltpu.make_async_copy(source, full.at[pl.ds(own_tokens, rows)], own.at[a])
        for a, (source, full) in enumerate(((x, xall), (ct, ctall)))
    ]

    def each_rep(step):
        for r in range(2):

            @pl.when(rep == r)
            def _():
                step(r)

    def y_step(r, item):
        if item[0] == "w":
            y_weights(*pieces[item[1]])
        else:
            y_tokens(item[1], item[2])

    def carried(n, r, owner):
        return owner * N_Y + (y if (r + n) % 2 == 0 else 1 - y)

    def own_send(slot):
        def step(r):
            n = ORDER[r][slot]
            u, w = pieces[n]
            if (r + n) % 2:
                wait(("yw", u, w), region(u, w, fs))
            src = region(u, w, carried(n, r, z))

            @pl.when(z < N_Z - 1)
            def _():
                start(("up", u, w, 1), src, src, to_up, lambda: z < N_Z - 1)

            @pl.when(z > 0)
            def _():
                start(("dn", u, w, 1), src, src, to_dn, lambda: z > 0)

        each_rep(step)

    def arrive(slot, d):
        def step(r):
            n = ORDER[r][slot]
            u, w = pieces[n]

            @pl.when(z - d >= 0)
            def _():
                src = region(u, w, carried(n, r, z - d))
                wait(("up", u, w, d), src)
                if d < N_Z - 1:

                    @pl.when(z < N_Z - 1)
                    def _():
                        start(
                            ("up", u, w, d + 1), src, src, to_up,
                            lambda: (z - d >= 0) & (z < N_Z - 1),
                        )

                start(("xw", u, w, N_Z - d), src, src, to_x)

            @pl.when(z + d <= N_Z - 1)
            def _():
                src = region(u, w, carried(n, r, z + d))
                wait(("dn", u, w, d), src)
                if d < N_Z - 1:

                    @pl.when(z > 0)
                    def _():
                        start(
                            ("dn", u, w, d + 1), src, src, to_dn,
                            lambda: (z + d <= N_Z - 1) & (z > 0),
                        )

                start(("xw", u, w, d), src, src, to_x)

        each_rep(step)

    def chunk_ready(u):
        for w in range(3):
            n = pieces.index((u, w))
            like = region(u, w, fs)

            @pl.when(rep == n % 2)
            def _():
                wait(("yw", u, w), like)

            for k in range(1, N_Z):
                wait(("xw", u, w, k), like)

    gain_row = gain[...]
    norm_rows = 64

    def normalize(first):
        def body(i, _):
            r = pl.ds(pl.multiple_of(first + i * norm_rows, norm_rows), norm_rows)
            single = xall[r, :].astype(F32)
            scale = lax.rsqrt(jnp.mean(single * single, axis=-1, keepdims=True) + EPS)
            inv[r, :] = scale
            xn[r, :] = (single * scale * gain_row).astype(BF16)
            return 0

        lax.fori_loop(0, rows // norm_rows, body, 0)

    def forward(u, first):
        r = pl.ds(first, rows)
        both = jnp.dot(xn[r, :], wgu[u], preferred_element_type=F32)
        gate, up = both[:, :uc], both[:, uc:]
        sig = jax.nn.sigmoid(gate)
        active = gate * sig
        hid[u, r, :] = (active * up).astype(BF16)
        d_hidden = 0.5 * jnp.dot(ctall[r, :], wd[u], preferred_element_type=F32)
        dgu[u, r, :uc] = (d_hidden * up * sig * (1.0 + gate * (1.0 - sig))).astype(BF16)
        dgu[u, r, uc:] = (d_hidden * active).astype(BF16)

    over_rows = (((0,), (0,)), ((), ()))
    over_cols = (((1,), (1,)), ((), ()))

    def down_terms(u):
        def body(zd, _):
            r = pl.ds(pl.multiple_of(zd * 2 * wrows, 2 * wrows), 2 * wrows)
            value = 0.5 * lax.dot_general(
                ctall[:, r], hid[u], over_rows, preferred_element_type=F32
            )
            dd32[u, zd] = value.reshape(2, 2, wrows // 2, uc)
            if u:
                ddb[u - 1, zd] = dd32[u, zd, :, 1 - rep].astype(BF16)
            return 0

        lax.fori_loop(0, N_Z, body, 0)

    def put(u, side, who, value):
        r = pl.ds(pl.multiple_of(side * (wrows // 2), wrows // 2), wrows // 2)
        c = pl.ds(pl.multiple_of(who * units + u * uc, uc), uc)
        ddv[r, c] = value.astype(F32)

    def first_to_z():
        zh[1] = dd32[0, z3].astype(BF16)
        start(("zh", 1), zh.at[1], zr.at[1], to_z[1])
        zh[0] = dd32[0, z1].astype(BF16)
        start(("zh", 0), zh.at[0], zr.at[0], to_z[1])

    def first_on_z():
        wait(("zh", 1), zr.at[1])
        zh[2] = (dd32[0, z2] + zr[1].astype(F32)).astype(BF16)
        start(("zh", 2), zh.at[2], zr.at[2], to_z[2])

    def first_to_x():
        wait(("zh", 0), zr.at[0])
        wait(("zh", 2), zr.at[2])
        total = dd32[0, z] + zr[0].astype(F32) + zr[2].astype(F32)
        hx[0] = total.astype(BF16)
        start(("hx",), hx.at[0], hx.at[1], to_x)

    def first_to_y():
        wait(("hx",), hx.at[1])
        total = (hx[0].astype(F32) + hx[1].astype(F32)).astype(BF16)
        zr[0] = total
        hy[0] = zr[0, 1 - y]
        start(("hy",), hy.at[0], hy.at[1], to_y)
        for side in range(2):
            put(0, side, y, zr[0, y, side])

    def first_final():
        wait(("hy",), hy.at[1])
        for side in range(2):
            put(0, side, 1 - y, hy[1, side])

    def down_to_x(u, ks=(3, 2, 1, 0)):
        for k in ks:
            zd = z if k == 0 else z_of[k]
            start(("rx", u, k), ddb.at[u - 1, zd], rx.at[u - 1, zd], to_x)

    def down_along_z(u, k):
        zd = z if k == 0 else z_of[k]
        wait(("rx", u, k), rx.at[u - 1, zd])
        total = dd32[u, zd, :, rep] + rx[u - 1, zd].astype(F32)
        if k == 0:
            fin[u - 1] = total
            return
        if k == 2:
            wait(("rz", u, 3), rz.at[u - 1, 3])
            total = total + rz[u - 1, 3].astype(F32)
        zs[u - 1, k] = total.astype(BF16)
        start(("rz", u, k), zs.at[u - 1, k], rz.at[u - 1, k], to_z[2 if k == 2 else 1])

    def down_final(u):
        total = fin[u - 1]
        for k in (1, 2):
            wait(("rz", u, k), rz.at[u - 1, k])
            total = total + rz[u - 1, k].astype(F32)
        zs[u - 1, 0] = total.astype(BF16)
        start(("ry", u), zs.at[u - 1, 0, 1 - y], ry.at[u - 1], to_y)
        start(("fx", u, 0), zs.at[u - 1, 0, y], fx.at[u - 1, 0], to_x)
        put(u, rep, y, zs[u - 1, 0, y])

    def down_y(u):
        wait(("ry", u), ry.at[u - 1])
        start(("fx", u, 1), ry.at[u - 1], fx.at[u - 1, 1], to_x)
        put(u, rep, 1 - y, ry[u - 1])

    def down_x(u):
        wait(("fx", u, 0), fx.at[u - 1, 0])
        put(u, 1 - rep, y, fx[u - 1, 0])
        wait(("fx", u, 1), fx.at[u - 1, 1])
        put(u, 1 - rep, 1 - y, fx[u - 1, 1])

    n_cols = 512

    def back(first, chunks, add=False):
        def body(j, _):
            c = pl.ds(pl.multiple_of(j * n_cols, n_cols), n_cols)
            total = dn[pl.ds(first, half), c] if add else None
            for u in chunks:
                term = lax.dot_general(
                    dgu[u, pl.ds(first, half), :], wgu[u, c, :], over_cols,
                    preferred_element_type=F32,
                )
                total = term if total is None else total + term
            dn[pl.ds(first, half), c] = total
            return 0

        lax.fori_loop(0, width // n_cols, body, 0)

    def back_to_core(h, first):
        r = pl.ds(pl.multiple_of(first + (1 - tp) * half, half), half)
        sd[h] = dn[r, :].astype(BF16)
        start(("cd", h), sd.at[h], rd.at[h], to_c)

    def half_of(first, who):
        return pl.multiple_of(first + who * half, half)

    bpart = half // BACK_PARTS

    def back_to_y(i):
        if i == 0:
            wait(("cd", 0), rd.at[0])
        r = pl.ds(pl.multiple_of(other_tokens + tp * half + i * bpart, bpart), bpart)
        q = pl.ds(i * bpart, bpart)
        mine = dn[r, :].astype(BF16).astype(F32)
        sy[q, :] = (mine + rd[0, q, :].astype(F32)).astype(BF16)
        start(("yd", i), sy.at[q], yd.at[q], to_y)

    def gain_terms(first):
        def body(i, acc):
            r = pl.ds(pl.multiple_of(first + i * norm_rows, norm_rows), norm_rows)
            terms = dn[r, :] * (xall[r, :].astype(F32) * inv[r, :])
            return acc + jnp.sum(terms.reshape(norm_rows // 8, 8, width), axis=0)

        return lax.fori_loop(0, rows // norm_rows, body, jnp.zeros((8, width), F32))

    gain_targets = (to_c, to_z[1], to_z[2], to_y, to_x)

    def gain_send(i):
        gsend[i] = gvec[...]
        start(("gg", i), gsend.at[i], grecv.at[i], gain_targets[i])

    def gain_recv(i):
        wait(("gg", i), grecv.at[i])
        gvec[...] = gvec[...] + grecv[i]

    out_row = pl.multiple_of(tp * half, half)

    def ig_copy(i):
        o = pl.ds(pl.multiple_of(out_row + i * bpart, bpart), bpart)
        return pltpu.make_async_copy(igv.at[o], ig.at[o], own.at[i])

    def dd_copy(u, who):
        c = pl.ds(who * units + u * uc, uc)
        return pltpu.make_async_copy(
            ddv.at[:, c], dd.at[:, c], own.at[BACK_PARTS + u * N_Y + who]
        )

    def dd_out(u):
        for who in range(N_Y):
            dd_copy(u, who).start()

    def back_final(i):
        q = pl.ds(i * bpart, bpart)
        wait(("yd", i), yd.at[q])
        r = pl.ds(pl.multiple_of(own_tokens + tp * half + i * bpart, bpart), bpart)
        mine = dn[r, :].astype(BF16).astype(F32) + rd[1, q, :].astype(F32)
        mine = mine.astype(BF16).astype(F32) + yd[q, :].astype(F32)
        mine = mine.astype(BF16).astype(F32)
        scale = inv[r, :]
        unit = xall[r, :].astype(F32) * scale
        scaled = gain_row * mine
        mean = jnp.mean(scaled * unit, axis=-1, keepdims=True)
        o = pl.ds(pl.multiple_of(out_row + i * bpart, bpart), bpart)
        igv[o, :] = (ctall[r, :].astype(F32) + scale * (scaled - unit * mean)).astype(BF16)
        start(("ig", i), igv.at[o], ig.at[o], to_c)
        ig_copy(i).start()

    likes = {
        "rx": rx.at[0, 0], "rz": rz.at[0, 0], "ry": ry.at[0], "fx": fx.at[0, 0],
        "cd": sd.at[0], "gg": grecv.at[0], "yd": yd.at[pl.ds(0, bpart)],
        "ig": igv.at[pl.ds(0, bpart)], "yt": xall.at[pl.ds(0, tpart)],
        "ct": xall.at[pl.ds(0, tpart)],
        "zh": zr.at[0], "hx": hx.at[0], "hy": hy.at[0],
    }

    def settle(early):
        for key, cond in list(pending.items()):
            if early and key[0] not in GATHER:
                continue
            del pending[key]
            like = likes[key[0]] if key[0] in likes else region(key[1], key[2], fs)
            if cond is None:
                remote(key, like, like, to_x).wait_send()
            else:

                @pl.when(cond())
                def _():
                    remote(key, like, like, to_x).wait_send()

    def y_upto(limit):
        def step(r):
            spent = 0
            for item in Y_ORDER[r]:
                cost = 1 if item[0] == "w" else 2
                if y_done[0] <= spent < limit:
                    y_step(r, item)
                spent += cost

        each_rep(step)
        y_done[0] = limit

    def core_token_group(a, parts):
        for i in parts:
            core_tokens(a, i)

    def tokens_ready(a):
        for i in range(TOKEN_PARTS):
            core_wait(a, i)

    y_done = [0]
    y_upto(1)
    for n in (0, 1, 2, 3):
        kept[n].start()
    kept_tokens[0].start()
    for n in range(4, len(pieces)):
        kept[n].start()
    kept_tokens[1].start()
    for n in (0, 1):
        kept[n].wait()
    own_send(0)
    kept_tokens[0].wait()
    y_upto(4)
    normalize(own_tokens)
    for copy in kept[2:] + kept_tokens[1:]:
        copy.wait()
    own_send(1)
    own_send(2)
    last = len(pieces)
    for t in range(last + 2):
        y_upto(3 * t + 7)
        if t + 2 < last and t + 2 >= 3:
            own_send(t + 2)
        for d in range(1, N_Z):
            if 0 <= t + 1 - d < last:
                arrive(t + 1 - d, d)
        if t == 2:
            core_token_group(0, (0, 1))
        if t == 4:
            core_token_group(0, (2, 3))
        if t == 5:
            tokens_ready(0)
            normalize(other_tokens)
        if t == 6:
            core_token_group(1, (0, 1))
            chunk_ready(0)
            forward(0, own_tokens)
        if t == 7:
            core_token_group(1, (2, 3))
        if t == 8:
            tokens_ready(1)
            forward(0, other_tokens)
        if t == 9:
            down_terms(0)
            first_to_z()
    chunk_ready(1)
    forward(1, own_tokens)
    forward(1, other_tokens)
    down_terms(1)
    down_to_x(1)
    early = tuple(range(CHUNKS - 1))
    final = CHUNKS - 1
    back(half_of(other_tokens, 1 - tp), early)
    back(half_of(other_tokens, tp), early)
    first_on_z()
    chunk_ready(final)
    forward(final, other_tokens)
    back(half_of(other_tokens, 1 - tp), (final,), True)
    back_to_core(0, other_tokens)
    down_along_z(1, 3)
    back(half_of(other_tokens, tp), (final,), True)
    for i in range(BACK_PARTS):
        back_to_y(i)
    down_along_z(1, 1)
    forward(2, own_tokens)
    down_terms(2)
    down_to_x(2)
    back(half_of(own_tokens, 1 - tp), range(CHUNKS))
    back_to_core(1, own_tokens)
    down_along_z(1, 2)
    down_along_z(1, 0)
    back(half_of(own_tokens, tp), range(CHUNKS))
    first_to_x()
    acc = gain_terms(own_tokens) + gain_terms(other_tokens)
    gvec[...] = jnp.sum(acc, axis=0, keepdims=True)
    gain_send(0)
    down_along_z(2, 3)
    wait(("cd", 1), rd.at[1])
    gain_recv(0)
    gain_send(1)
    down_along_z(2, 1)
    down_final(1)
    back_final(0)
    back_final(1)
    down_along_z(2, 2)
    down_along_z(2, 0)
    settle(True)
    back_final(2)
    gain_recv(1)
    gain_send(2)
    back_final(3)
    back_final(4)
    down_final(2)
    back_final(5)
    gain_recv(2)
    gain_send(3)
    first_to_y()
    down_y(1)
    back_final(6)
    back_final(7)
    gain_recv(3)
    gain_send(4)
    down_y(2)
    down_x(1)
    dd_out(1)
    first_final()
    dd_out(0)
    down_x(2)
    dd_out(2)
    gain_recv(4)
    for i in range(BACK_PARTS):
        o = pl.ds(pl.multiple_of(i * bpart, bpart), bpart)
        wait(("ig", i), igv.at[o])
    gg_copy = pltpu.make_async_copy(gvec, gg, own.at[BACK_PARTS + N_Y * CHUNKS])
    gg_copy.start()
    settle(False)
    for i in range(BACK_PARTS):
        ig_copy(i).wait()
    for u in range(CHUNKS):
        for who in range(N_Y):
            dd_copy(u, who).wait()
    gg_copy.wait()


def fused(x, gain, gate_w, up_w, down_w, ct):
    rows, width = x.shape
    wrows, cols = gate_w.shape
    units = cols // N_Y
    uc = units // CHUNKS
    half = rows // 2
    n = len(all_slots().slots)
    vm = pltpu.VMEM
    anywhere = pl.BlockSpec(memory_space=pl.ANY)
    tile = (2, wrows // 2, uc)
    ig, gg, dd = pl.pallas_call(
        fused_kernel,
        out_shape=[
            jax.ShapeDtypeStruct((rows, width), BF16),
            jax.ShapeDtypeStruct((1, width), F32),
            jax.ShapeDtypeStruct((wrows, cols), F32),
        ],
        in_specs=[anywhere, pl.BlockSpec(memory_space=vm)] + [anywhere] * 4,
        out_specs=[anywhere] * 3,
        scratch_shapes=[
            vm((CHUNKS, width, 2 * uc), BF16),
            vm((CHUNKS, width, uc), BF16),
            vm((2 * rows, width), BF16),
            vm((2 * rows, width), BF16),
            vm((2 * rows, width), BF16),
            vm((2 * rows, 1), F32),
            vm((CHUNKS, 2 * rows, uc), BF16),
            vm((CHUNKS, 2 * rows, 2 * uc), BF16),
            vm((2 * rows, width), F32),
            vm((CHUNKS, N_Z, 2) + tile, F32),
            vm((CHUNKS - 1, N_Z) + tile, BF16),
            vm((CHUNKS - 1, N_Z) + tile, BF16),
            vm((CHUNKS - 1, N_Z) + tile, BF16),
            vm((CHUNKS - 1, N_Z) + tile, BF16),
            vm((CHUNKS - 1,) + tile, F32),
            vm((CHUNKS - 1,) + tile[1:], BF16),
            vm((CHUNKS - 1,) + tile, BF16),
            vm((2, half, width), BF16),
            vm((2, half, width), BF16),
            vm((half, width), BF16),
            vm((half, width), BF16),
            vm((rows, width), BF16),
            vm((5, 1, width), F32),
            vm((5, 1, width), F32),
            vm((wrows, cols), F32),
            vm((1, width), F32),
            vm((3, 2) + tile, BF16),
            vm((3, 2) + tile, BF16),
            vm((2, 2) + tile, BF16),
            vm((2,) + tile, BF16),
            pltpu.SemaphoreType.DMA((n,)),
            pltpu.SemaphoreType.DMA((n,)),
            pltpu.SemaphoreType.DMA((BACK_PARTS + N_Y * CHUNKS + 2,)),
        ],
        compiler_params=pltpu.CompilerParams(
            collective_id=0, has_side_effects=True, vmem_limit_bytes=67043328
        ),
        name="fused",
    )(x, gain.reshape(1, width), gate_w, up_w, down_w, ct)
    return ig, gg.reshape(width), dd


def shift(value, axis, step):
    size = lax.axis_size(axis)
    return lax.ppermute(value, axis, [(i, (i + step) % size) for i in range(size)])


def swap(value, axis, bit):
    return lax.ppermute(value, axis, [(i, i ^ bit) for i in range(lax.axis_size(axis))])


def summed_everywhere(value):
    for axis in ("rep", "fs", "tp"):
        size = lax.axis_size(axis)
        if size & (size - 1):
            value = lax.psum(value, axis)
            continue
        bit = 1
        while bit < size:
            value = value + swap(value, axis, bit)
            bit *= 2
    return value


def local(inputs, gain, gate_weight, up_weight, down_weight, cotangent):
    n_rep, n_tp = lax.axis_size("rep"), lax.axis_size("tp")
    if (n_rep, lax.axis_size("fs"), n_tp) == (2, N_Y * N_Z, 2):
        return fused(inputs, gain, gate_weight, up_weight, down_weight, cotangent)
    rep, tp = lax.axis_index("rep"), lax.axis_index("tp")
    rows, width = inputs.shape
    block = rows // n_tp
    units = gate_weight.shape[1] // n_rep

    def own_units(weight):
        return lax.dynamic_slice_in_dim(weight, rep * units, units, axis=1)

    def own_block(value, step):
        return lax.dynamic_slice_in_dim(value, (tp + step) % n_tp * block, block, axis=0)

    def gathered_tokens(value):
        parts = [own_block(value, s) for s in range(n_tp)]
        for j in range(1, n_rep):
            first = shift(own_block(value, 0), "rep", -j)
            parts += [first] + [shift(first, "tp", -s) for s in range(1, n_tp)]
        return jnp.concatenate(parts, axis=0)

    both_own = jnp.concatenate([own_units(gate_weight), own_units(up_weight)], axis=1)
    both_full = lax.all_gather(both_own, "fs", axis=0, tiled=True)
    down_full = lax.all_gather(own_units(down_weight), "fs", axis=0, tiled=True)
    tokens = gathered_tokens(inputs)
    cots = gathered_tokens(cotangent)

    def normed(value):
        single = value.astype(jnp.float32)
        inv = lax.rsqrt(jnp.mean(single * single, axis=-1, keepdims=True) + EPS)
        return single * inv, inv

    normalized_input = (normed(tokens)[0] * gain).astype(jnp.bfloat16)
    contract_cols = (((1,), (1,)), ((), ()))
    contract_rows = (((0,), (0,)), ((), ()))
    both = jnp.dot(normalized_input, both_full, preferred_element_type=jnp.float32)
    gate, up_proj = both[:, :units], both[:, units:]
    gate_sig = jax.nn.sigmoid(gate)
    active = gate * gate_sig
    hidden = (active * up_proj).astype(jnp.bfloat16)
    d_down_terms = (
        0.5 * lax.dot_general(cots, hidden, contract_rows, preferred_element_type=jnp.float32)
    ).astype(jnp.bfloat16)
    d_down_terms, cots = lax.optimization_barrier((d_down_terms, cots))
    summed = lax.psum_scatter(d_down_terms, "fs", scatter_dimension=0, tiled=True)
    d_hidden = 0.5 * jnp.dot(cots, down_full, preferred_element_type=jnp.float32)
    d_gate = (d_hidden * up_proj * gate_sig * (1.0 + gate * (1.0 - gate_sig))).astype(jnp.bfloat16)
    d_up = (d_hidden * active).astype(jnp.bfloat16)
    partial_value = (
        lax.dot_general(
            jnp.concatenate([d_gate, d_up], axis=1),
            both_full,
            contract_cols,
            preferred_element_type=jnp.float32,
        )
    ).astype(jnp.bfloat16).reshape(n_rep, n_tp, block, width)

    def tp_terms(step):
        return partial_value[:, step]

    over_tp = tp_terms(0).astype(jnp.float32)
    for s in range(1, n_tp):
        over_tp = over_tp + shift(tp_terms(s), "tp", s).astype(jnp.float32)
    over_tp = over_tp.astype(jnp.bfloat16)
    total = over_tp[0].astype(jnp.float32)
    for j in range(1, n_rep):
        total = total + shift(over_tp[j], "rep", j).astype(jnp.float32)
    normalized_gradient = total.astype(jnp.bfloat16).astype(jnp.float32)
    unit_input, inv = normed(own_block(inputs, 0))
    gain_gradient = summed_everywhere(jnp.sum(normalized_gradient * unit_input, axis=0))
    gain_scaled = gain * normalized_gradient
    mean_correction = jnp.mean(gain_scaled * unit_input, axis=-1, keepdims=True)
    block_gradient = (
        own_block(cotangent, 0).astype(jnp.float32)
        + inv * (gain_scaled - unit_input * mean_correction)
    ).astype(jnp.bfloat16)
    input_gradient = jnp.zeros((rows, width), jnp.bfloat16)
    for s in range(n_tp):
        piece = block_gradient if s == 0 else shift(block_gradient, "tp", -s)
        input_gradient = lax.dynamic_update_slice_in_dim(
            input_gradient, piece, (tp + s) % n_tp * block, axis=0
        )
    d_down = jnp.zeros((summed.shape[0], units * n_rep), jnp.float32)
    for j in range(n_rep):
        piece = summed if j == 0 else shift(summed, "rep", -j)
        d_down = lax.dynamic_update_slice_in_dim(
            d_down, piece.astype(jnp.float32), (rep + j) % n_rep * units, axis=1
        )
    return (input_gradient, gain_gradient, d_down)


def solution(mesh):
    placed = (
        P(("rep", "fs"), None),
        P(),
        P("fs", "tp"),
        P("fs", "tp"),
        P("fs", "tp"),
        P(("rep", "fs"), None),
    )
    return jax.shard_map(
        local,
        mesh=mesh,
        in_specs=placed,
        out_specs=(P(("rep", "fs"), None), P(), P("fs", "tp")),
        check_vma=False,
    )
```

```python
import jax
import jax.numpy as jnp
from jax import lax
from jax.experimental import pallas as pl
from jax.experimental.pallas import tpu as pltpu
from jax.sharding import PartitionSpec as P

EPS = 1e-06
F32, BF16 = jnp.float32, jnp.bfloat16
MESH_ID = pl.DeviceIdType.MESH
N_Y, N_Z = 2, 4
CHUNKS = 3
TOKEN_PARTS = 4
BACK_PARTS = 8


ORDER = ((0, 2, 1, 4, 3, 5, 6, 7, 8), (1, 3, 0, 2, 5, 4, 7, 6, 8))
Y_ORDER = tuple(
    tuple(("w", i) if isinstance(i, int) else ("t",) + i for i in order)
    for order in (
        (1, (0, 0), 3, (0, 1), 5, (0, 2), (0, 3), 0, 2, 7, (1, 0), (1, 1), (1, 2), (1, 3), 4, 6, 8),
        (0, 2, (0, 0), (0, 1), 4, (0, 2), (0, 3), 1, 6, (1, 0), 8, (1, 1), (1, 2), (1, 3), 3, 5, 7),
    )
)


SEND_GROUPS = {"yw": 0, "yt": 0, "ct": 0, "xw": 1, "up": 2, "dn": 3, "gc": 4, "gp": 4, "gz": 4}
LATE = 5
MERGED = {"xw": 2, "ct": 2, "ig": 1, "gp": 1, "gz": 1, "fx": 2}


def arrival(key):
    name = key[0]
    if name == "up":
        return ("zw", key[1], key[2], N_Z - key[3])
    if name == "dn":
        return ("zw",) + key[1:]
    if name == "rz":
        return ("rz", key[1], min(key[2] // 2, 1)) if key[2] > 2 else ("rz", key[1], 0)
    return key[: MERGED.get(name, len(key))]


def all_slots():
    keys = []
    for u in range(CHUNKS):
        keys.append(("xw", u))
        for w in range(3):
            keys.append(("yw", u, w))
            keys += [("zw", u, w, k) for k in range(1, N_Z)]
        if u:
            keys += [("rx", u, k) for k in range(N_Z)]
            keys += [("rz", u, 0), ("rz", u, 1), ("ry", u), ("fx", u)]
    keys += [("zh", i) for i in range(3)] + [("hx",), ("hy",)]
    for a in range(2):
        keys += [("yt", a, i) for i in range(TOKEN_PARTS)] + [("ct", a), ("cd", a)]
    keys += [("yd", i) for i in range(BACK_PARTS)]
    keys += [("ig",), ("gc",), ("gp",), ("gz",)]
    return {key: i for i, key in enumerate(keys)}


def fused_kernel(
    x, gain, gate_w, up_w, down_w, ct,
    ig, gg, dd,
    wgu, wd, xall, ctall, xn, inv, hid, dgu, dn, dd32, ddb, rx, zs, rz, fin, ry, fx,
    sd, rd, sy, yd, igv, gp, gz, ddv, gvec, zh, zr, hx, hy,
    send, recv, own,
):
    slots = all_slots()
    rep, fs, tp = lax.axis_index("rep"), lax.axis_index("fs"), lax.axis_index("tp")
    z, y = fs // N_Y, fs % N_Y
    rows, width = x.shape
    wrows, cols = gate_w.shape
    units = cols // N_Y
    uc = units // CHUNKS
    half = rows // 2
    to_x, to_c = {"rep": 1 - rep}, {"tp": 1 - tp}
    to_y = {"fs": z * N_Y + 1 - y}
    to_xy = {"rep": 1 - rep, "fs": z * N_Y + 1 - y}
    to_up, to_dn = {"fs": fs + N_Y}, {"fs": fs - N_Y}
    z1 = z + 1 - 2 * (z % 2)
    z2 = (z + 2) % N_Z
    z3 = N_Z - 1 - z
    to_z = {1: {"fs": z1 * N_Y + y}, 2: {"fs": z2 * N_Y + y}, 3: {"fs": z3 * N_Y + y}}
    z_of = {1: z1, 2: z2, 3: z3}

    barrier = pltpu.get_barrier_semaphore()
    for target in (to_x, to_c, to_y, to_xy, to_z[1], to_z[2], to_z[3]):
        pl.semaphore_signal(barrier, inc=1, device_id=target, device_id_type=MESH_ID)
    pl.semaphore_wait(barrier, 7)

    def remote(key, src, dst, target):
        return pltpu.make_async_remote_copy(
            src_ref=src, dst_ref=dst,
            send_sem=send.at[SEND_GROUPS.get(key[0], LATE)],
            recv_sem=recv.at[slots[arrival(key)]],
            device_id=target, device_id_type=MESH_ID,
        )

    def start(key, src, dst, target):
        remote(key, src, dst, target).start()

    def wait(key, like):
        remote(key, like, like, to_x).wait_recv()

    tall = wrows * uc * 2 // (width * 4)

    def span(count):
        return dn.at[pl.ds(0, count * tall)]

    def sent(name, like):
        group = SEND_GROUPS.get(name, LATE)
        pltpu.make_async_remote_copy(
            src_ref=like, dst_ref=like, send_sem=send.at[group],
            recv_sem=recv.at[0], device_id=to_x, device_id_type=MESH_ID,
        ).wait_send()

    def region(u, w, owner):
        r = pl.ds(pl.multiple_of(owner * wrows, wrows), wrows)
        if w == 2:
            return wd.at[u, r]
        return wgu.at[u, r, pl.ds(w * uc, uc)]

    weights = (gate_w, up_w, down_w)

    def part(w, who, u):
        return weights[w].at[:, pl.ds(pl.multiple_of(who * units + u * uc, uc), uc)]

    def y_weights(u, w):
        start(("yw", u, w), part(w, 1 - y, u), region(u, w, fs), to_y)

    own_tokens = pl.multiple_of(y * rows, rows)
    other_tokens = pl.multiple_of((1 - y) * rows, rows)
    tpart = half // TOKEN_PARTS

    def y_tokens(a, i):
        full = (xall, ctall)[a]
        r = pl.ds(pl.multiple_of(own_tokens + tp * half + i * tpart, tpart), tpart)
        start(("yt", a, i), full.at[r], full.at[r], to_y)

    def core_tokens(a, i):
        full = (xall, ctall)[a]
        r = pl.ds(pl.multiple_of(other_tokens + tp * half + i * tpart, tpart), tpart)
        wait(("yt", a, i), full.at[r])
        start(("ct", a, i), full.at[r], full.at[r], to_c)

    pieces = [(u, w) for u in range(CHUNKS) for w in range(3)]

    def local_copy(n):
        u, w = pieces[n]
        return pltpu.make_async_copy(part(w, y, u), region(u, w, fs), own.at[2 + n])

    kept = [local_copy(n) for n in range(len(pieces))]
    kept_tokens = [
        pltpu.make_async_copy(source, full.at[pl.ds(own_tokens, rows)], own.at[a])
        for a, (source, full) in enumerate(((x, xall), (ct, ctall)))
    ]

    def each_rep(step):
        for r in range(2):

            @pl.when(rep == r)
            def _():
                step(r)

    def y_step(r, item):
        if item[0] == "w":
            y_weights(*pieces[item[1]])
        else:
            y_tokens(item[1], item[2])

    def carried(n, r, owner):
        return owner * N_Y + (y if (r + n) % 2 == 0 else 1 - y)

    def own_send(slot):
        def step(r):
            n = ORDER[r][slot]
            u, w = pieces[n]
            if (r + n) % 2:
                wait(("yw", u, w), region(u, w, fs))
            src = region(u, w, carried(n, r, z))

            @pl.when(z < N_Z - 1)
            def _():
                start(("up", u, w, 1), src, src, to_up)

            @pl.when(z > 0)
            def _():
                start(("dn", u, w, 1), src, src, to_dn)

        each_rep(step)

    def arrive(slot, d):
        def step(r):
            n = ORDER[r][slot]
            u, w = pieces[n]

            @pl.when(z - d >= 0)
            def _():
                src = region(u, w, carried(n, r, z - d))
                wait(("up", u, w, d), src)
                if d < N_Z - 1:

                    @pl.when(z < N_Z - 1)
                    def _():
                        start(("up", u, w, d + 1), src, src, to_up)

                start(("xw", u, w, N_Z - d), src, src, to_x)

            @pl.when(z + d <= N_Z - 1)
            def _():
                src = region(u, w, carried(n, r, z + d))
                wait(("dn", u, w, d), src)
                if d < N_Z - 1:

                    @pl.when(z > 0)
                    def _():
                        start(("dn", u, w, d + 1), src, src, to_dn)

                start(("xw", u, w, d), src, src, to_x)

        each_rep(step)

    def chunk_ready(u):
        for w in range(3):
            n = pieces.index((u, w))
            like = region(u, w, fs)

            @pl.when(rep == n % 2)
            def _():
                wait(("yw", u, w), like)

        wait(("xw", u), span(3 * (N_Z - 1)))

    gain_row = gain[...]
    norm_rows = 64

    def normalize(first):
        def body(i, _):
            r = pl.ds(pl.multiple_of(first + i * norm_rows, norm_rows), norm_rows)
            single = xall[r, :].astype(F32)
            scale = lax.rsqrt(jnp.mean(single * single, axis=-1, keepdims=True) + EPS)
            inv[r, :] = scale
            xn[r, :] = (single * scale * gain_row).astype(BF16)
            return 0

        lax.fori_loop(0, rows // norm_rows, body, 0)

    def forward(u, first):
        r = pl.ds(first, rows)
        both = jnp.dot(xn[r, :], wgu[u], preferred_element_type=F32)
        gate, up = both[:, :uc], both[:, uc:]
        sig = jax.nn.sigmoid(gate)
        active = gate * sig
        hid[u, r, :] = (active * up).astype(BF16)
        d_hidden = 0.5 * jnp.dot(ctall[r, :], wd[u], preferred_element_type=F32)
        dgu[u, r, :uc] = (d_hidden * up * sig * (1.0 + gate * (1.0 - sig))).astype(BF16)
        dgu[u, r, uc:] = (d_hidden * active).astype(BF16)

    over_rows = (((0,), (0,)), ((), ()))
    over_cols = (((1,), (1,)), ((), ()))

    def down_terms(u):
        def body(zd, _):
            r = pl.ds(pl.multiple_of(zd * 2 * wrows, 2 * wrows), 2 * wrows)
            value = 0.5 * lax.dot_general(
                ctall[:, r], hid[u], over_rows, preferred_element_type=F32
            )
            dd32[u, zd] = value.reshape(2, 2, wrows // 2, uc)
            if u:
                ddb[u - 1, zd] = dd32[u, zd, :, 1 - rep].astype(BF16)
            return 0

        lax.fori_loop(0, N_Z, body, 0)

    def put(u, side, who, value):
        r = pl.ds(pl.multiple_of(side * (wrows // 2), wrows // 2), wrows // 2)
        c = pl.ds(pl.multiple_of(who * units + u * uc, uc), uc)
        ddv[r, c] = value.astype(F32)

    def first_to_z():
        zh[1] = dd32[0, z3].astype(BF16)
        start(("zh", 1), zh.at[1], zr.at[1], to_z[1])
        zh[0] = dd32[0, z1].astype(BF16)
        start(("zh", 0), zh.at[0], zr.at[0], to_z[1])

    def first_on_z():
        wait(("zh", 1), zr.at[1])
        zh[2] = (dd32[0, z2] + zr[1].astype(F32)).astype(BF16)
        start(("zh", 2), zh.at[2], zr.at[2], to_z[2])

    def first_to_x():
        wait(("zh", 0), zr.at[0])
        wait(("zh", 2), zr.at[2])
        total = dd32[0, z] + zr[0].astype(F32) + zr[2].astype(F32)
        hx[0] = total.astype(BF16)
        start(("hx",), hx.at[0], hx.at[1], to_x)

    def first_to_y():
        wait(("hx",), hx.at[1])
        total = (hx[0].astype(F32) + hx[1].astype(F32)).astype(BF16)
        zr[0] = total
        hy[0] = zr[0, 1 - y]
        start(("hy",), hy.at[0], hy.at[1], to_y)
        for side in range(2):
            put(0, side, y, zr[0, y, side])

    def first_final():
        wait(("hy",), hy.at[1])
        for side in range(2):
            put(0, side, 1 - y, hy[1, side])

    def down_to_x(u, ks=(3, 2, 1, 0)):
        for k in ks:
            zd = z if k == 0 else z_of[k]
            start(("rx", u, k), ddb.at[u - 1, zd], rx.at[u - 1, zd], to_x)

    def down_along_z(u, k):
        zd = z if k == 0 else z_of[k]
        wait(("rx", u, k), rx.at[u - 1, zd])
        total = dd32[u, zd, :, rep] + rx[u - 1, zd].astype(F32)
        if k == 0:
            fin[u - 1] = total
            return
        if k == 2:
            wait(("rz", u, 3), rz.at[u - 1, 3])
            total = total + rz[u - 1, 3].astype(F32)
        zs[u - 1, k] = total.astype(BF16)
        start(("rz", u, k), zs.at[u - 1, k], rz.at[u - 1, k], to_z[2 if k == 2 else 1])

    def down_final(u):
        total = fin[u - 1]
        wait(("rz", u, 1), rz.at[u - 1, pl.ds(1, 2)])
        for k in (1, 2):
            total = total + rz[u - 1, k].astype(F32)
        zs[u - 1, 0] = total.astype(BF16)
        start(("ry", u), zs.at[u - 1, 0, 1 - y], ry.at[u - 1], to_y)
        start(("fx", u, 1), zs.at[u - 1, 0, 1 - y], fx.at[u - 1, 1], to_xy)
        start(("fx", u, 0), zs.at[u - 1, 0, y], fx.at[u - 1, 0], to_x)
        put(u, rep, y, zs[u - 1, 0, y])

    def down_y(u):
        wait(("ry", u), ry.at[u - 1])
        put(u, rep, 1 - y, ry[u - 1])

    def down_x(u):
        wait(("fx", u), fx.at[u - 1])
        put(u, 1 - rep, y, fx[u - 1, 0])
        put(u, 1 - rep, 1 - y, fx[u - 1, 1])

    n_cols = 512

    def back(first, chunks, add=False):
        def body(j, _):
            c = pl.ds(pl.multiple_of(j * n_cols, n_cols), n_cols)
            total = dn[pl.ds(first, half), c] if add else None
            for u in chunks:
                term = lax.dot_general(
                    dgu[u, pl.ds(first, half), :], wgu[u, c, :], over_cols,
                    preferred_element_type=F32,
                )
                total = term if total is None else total + term
            dn[pl.ds(first, half), c] = total
            return 0

        lax.fori_loop(0, width // n_cols, body, 0)

    def back_to_core(h, first):
        r = pl.ds(pl.multiple_of(first + (1 - tp) * half, half), half)
        sd[h] = dn[r, :].astype(BF16)
        start(("cd", h), sd.at[h], rd.at[h], to_c)

    def half_of(first, who):
        return pl.multiple_of(first + who * half, half)

    bpart = half // BACK_PARTS

    def back_to_y(i):
        if i == 0:
            wait(("cd", 0), rd.at[0])
        r = pl.ds(pl.multiple_of(other_tokens + tp * half + i * bpart, bpart), bpart)
        q = pl.ds(i * bpart, bpart)
        mine = dn[r, :].astype(BF16).astype(F32)
        sy[q, :] = (mine + rd[0, q, :].astype(F32)).astype(BF16)
        start(("yd", i), sy.at[q], yd.at[q], to_y)

    def gain_terms(first):
        def body(i, acc):
            r = pl.ds(pl.multiple_of(first + i * norm_rows, norm_rows), norm_rows)
            terms = dn[r, :] * (xall[r, :].astype(F32) * inv[r, :])
            return acc + jnp.sum(terms.reshape(norm_rows // 8, 8, width), axis=0)

        return lax.fori_loop(0, rows // norm_rows, body, jnp.zeros((8, width), F32))

    in_plane = rep * N_Y + y

    def gain_core():
        acc = gain_terms(own_tokens) + gain_terms(other_tokens)
        gvec[0] = jnp.sum(acc, axis=0, keepdims=True)
        start(("gc",), gvec.at[0], gvec.at[1], to_c)

    def gain_plane():
        wait(("gc",), gvec.at[1])
        gp[in_plane] = gvec[0] + gvec[1]
        here = gp.at[in_plane]
        for i, target in enumerate((to_y, to_x, to_xy)):
            start(("gp", i), here, here, target)

    def gain_z():
        wait(("gp",), gp.at[pl.ds(0, 3)])
        gz[z] = gp[0] + gp[1] + gp[2] + gp[3]
        for i in range(3):
            start(("gz", i), gz.at[z], gz.at[z], to_z[i + 1])

    def gain_end():
        wait(("gz",), gz.at[pl.ds(0, 3)])
        gvec[2] = gz[0] + gz[1] + gz[2] + gz[3]

    out_row = pl.multiple_of(tp * half, half)

    def ig_copy(i):
        o = pl.ds(pl.multiple_of(out_row + i * bpart, bpart), bpart)
        return pltpu.make_async_copy(igv.at[o], ig.at[o], own.at[i])

    def dd_copy(u, who):
        c = pl.ds(who * units + u * uc, uc)
        return pltpu.make_async_copy(
            ddv.at[:, c], dd.at[:, c], own.at[BACK_PARTS + u * N_Y + who]
        )

    def dd_out(u):
        for who in range(N_Y):
            dd_copy(u, who).start()

    def back_final(i):
        q = pl.ds(i * bpart, bpart)
        wait(("yd", i), yd.at[q])
        r = pl.ds(pl.multiple_of(own_tokens + tp * half + i * bpart, bpart), bpart)
        mine = dn[r, :].astype(BF16).astype(F32) + rd[1, q, :].astype(F32)
        mine = mine.astype(BF16).astype(F32) + yd[q, :].astype(F32)
        mine = mine.astype(BF16).astype(F32)
        scale = inv[r, :]
        unit = xall[r, :].astype(F32) * scale
        scaled = gain_row * mine
        mean = jnp.mean(scaled * unit, axis=-1, keepdims=True)
        o = pl.ds(pl.multiple_of(out_row + i * bpart, bpart), bpart)
        igv[o, :] = (ctall[r, :].astype(F32) + scale * (scaled - unit * mean)).astype(BF16)
        start(("ig", i), igv.at[o], ig.at[o], to_c)
        ig_copy(i).start()

    def gather_sent():
        sent("yw", span(3 * CHUNKS + 2 * TOKEN_PARTS * 2 * 2))
        sent("xw", span(3 * CHUNKS * (N_Z - 1)))
        for i in range(N_Z - 1):

            @pl.when(z == i)
            def _():
                sent("up", span(3 * CHUNKS * (i + 1)))

            @pl.when(z == N_Z - 1 - i)
            def _():
                sent("dn", span(3 * CHUNKS * (i + 1)))

    def y_upto(limit):
        def step(r):
            spent = 0
            for item in Y_ORDER[r]:
                cost = 1 if item[0] == "w" else 2
                if y_done[0] <= spent < limit:
                    y_step(r, item)
                spent += cost

        each_rep(step)
        y_done[0] = limit

    def core_token_group(a, parts):
        for i in parts:
            core_tokens(a, i)

    def tokens_ready(a):
        wait(("ct", a), (xall, ctall)[a].at[pl.ds(0, half)])

    y_done = [0]
    y_upto(1)
    for n in (0, 1, 2, 3):
        kept[n].start()
    kept_tokens[0].start()
    for n in range(4, len(pieces)):
        kept[n].start()
    kept_tokens[1].start()
    for n in (0, 1):
        kept[n].wait()
    own_send(0)
    kept_tokens[0].wait()
    y_upto(4)
    normalize(own_tokens)
    for copy in kept[2:] + kept_tokens[1:]:
        copy.wait()
    own_send(1)
    own_send(2)
    last = len(pieces)
    for t in range(last + 2):
        y_upto(3 * t + 7)
        if t + 2 < last and t + 2 >= 3:
            own_send(t + 2)
        for d in range(1, N_Z):
            if t == 8 and d == 3:
                tokens_ready(1)
                forward(0, other_tokens)
            if t == 9 and d == 3:
                first_to_z()
                chunk_ready(1)
                forward(1, own_tokens)
            if 0 <= t + 1 - d < last:
                arrive(t + 1 - d, d)
        if t == 2:
            core_token_group(0, (0, 1))
        if t == 4:
            core_token_group(0, (2, 3))
        if t == 5:
            tokens_ready(0)
            normalize(other_tokens)
        if t == 6:
            core_token_group(1, (0, 1))
            chunk_ready(0)
            forward(0, own_tokens)
        if t == 7:
            core_token_group(1, (2, 3))
        if t == 8:
            down_terms(0)
    forward(1, other_tokens)
    down_terms(1)
    down_to_x(1)
    early = tuple(range(CHUNKS - 1))
    final = CHUNKS - 1
    back(half_of(other_tokens, 1 - tp), early)
    back(half_of(other_tokens, tp), early)
    chunk_ready(final)
    forward(final, other_tokens)
    back(half_of(other_tokens, 1 - tp), (final,), True)
    back_to_core(0, other_tokens)
    first_on_z()
    down_along_z(1, 3)
    back(half_of(other_tokens, tp), (final,), True)
    for i in range(BACK_PARTS - 2):
        back_to_y(i)
    down_along_z(1, 1)
    forward(2, own_tokens)
    down_terms(2)
    down_to_x(2)
    back(half_of(own_tokens, 1 - tp), range(CHUNKS))
    back_to_core(1, own_tokens)
    down_along_z(1, 2)
    down_along_z(1, 0)
    back(half_of(own_tokens, tp), range(CHUNKS))
    gain_core()
    down_along_z(2, 3)
    gain_plane()
    for i in range(BACK_PARTS - 2, BACK_PARTS):
        back_to_y(i)
    first_to_x()
    wait(("cd", 1), rd.at[1])
    down_along_z(2, 1)
    down_final(1)
    back_final(0)
    back_final(1)
    down_along_z(2, 2)
    down_along_z(2, 0)
    gather_sent()
    gain_z()
    back_final(2)
    back_final(3)
    back_final(4)
    back_final(5)
    first_to_y()
    down_final(2)
    down_y(1)
    back_final(6)
    back_final(7)
    down_x(1)
    dd_out(1)
    gain_end()
    gg_copy = pltpu.make_async_copy(gvec.at[2], gg, own.at[BACK_PARTS + N_Y * CHUNKS])
    gg_copy.start()
    first_final()
    dd_out(0)
    down_y(2)
    down_x(2)
    dd_out(2)
    wait(("ig",), igv.at[pl.ds(0, half)])
    rest = (CHUNKS - 1) * (N_Z + N_Z - 1) + 3 * (CHUNKS - 1) // 2 + 3 * 2 + 2 + 1
    moved = 2 * half * width // (wrows * uc)
    sent("late", span(rest + 2 * moved))
    sent("gc", gp.at[pl.ds(0, 7)])
    for i in range(BACK_PARTS):
        ig_copy(i).wait()
    for u in range(CHUNKS):
        for who in range(N_Y):
            dd_copy(u, who).wait()
    gg_copy.wait()


def fused(x, gain, gate_w, up_w, down_w, ct):
    rows, width = x.shape
    wrows, cols = gate_w.shape
    units = cols // N_Y
    uc = units // CHUNKS
    half = rows // 2
    n = len(all_slots())
    vm = pltpu.VMEM
    anywhere = pl.BlockSpec(memory_space=pl.ANY)
    tile = (2, wrows // 2, uc)
    ig, gg, dd = pl.pallas_call(
        fused_kernel,
        out_shape=[
            jax.ShapeDtypeStruct((rows, width), BF16),
            jax.ShapeDtypeStruct((1, width), F32),
            jax.ShapeDtypeStruct((wrows, cols), F32),
        ],
        in_specs=[anywhere, pl.BlockSpec(memory_space=vm)] + [anywhere] * 4,
        out_specs=[anywhere] * 3,
        scratch_shapes=[
            vm((CHUNKS, width, 2 * uc), BF16),
            vm((CHUNKS, width, uc), BF16),
            vm((2 * rows, width), BF16),
            vm((2 * rows, width), BF16),
            vm((2 * rows, width), BF16),
            vm((2 * rows, 1), F32),
            vm((CHUNKS, 2 * rows, uc), BF16),
            vm((CHUNKS, 2 * rows, 2 * uc), BF16),
            vm((2 * rows, width), F32),
            vm((CHUNKS, N_Z, 2) + tile, F32),
            vm((CHUNKS - 1, N_Z) + tile, BF16),
            vm((CHUNKS - 1, N_Z) + tile, BF16),
            vm((CHUNKS - 1, N_Z) + tile, BF16),
            vm((CHUNKS - 1, N_Z) + tile, BF16),
            vm((CHUNKS - 1,) + tile, F32),
            vm((CHUNKS - 1,) + tile[1:], BF16),
            vm((CHUNKS - 1,) + tile, BF16),
            vm((2, half, width), BF16),
            vm((2, half, width), BF16),
            vm((half, width), BF16),
            vm((half, width), BF16),
            vm((rows, width), BF16),
            vm((8, 1, width), F32),
            vm((N_Z, 1, width), F32),
            vm((wrows, cols), F32),
            vm((3, 1, width), F32),
            vm((3, 2) + tile, BF16),
            vm((3, 2) + tile, BF16),
            vm((2, 2) + tile, BF16),
            vm((2,) + tile, BF16),
            pltpu.SemaphoreType.DMA((LATE + 1,)),
            pltpu.SemaphoreType.DMA((n,)),
            pltpu.SemaphoreType.DMA((BACK_PARTS + N_Y * CHUNKS + 2,)),
        ],
        compiler_params=pltpu.CompilerParams(
            collective_id=0, has_side_effects=True, vmem_limit_bytes=67043328
        ),
        name="fused",
    )(x, gain.reshape(1, width), gate_w, up_w, down_w, ct)
    return ig, gg.reshape(width), dd


def shift(value, axis, step):
    size = lax.axis_size(axis)
    return lax.ppermute(value, axis, [(i, (i + step) % size) for i in range(size)])


def swap(value, axis, bit):
    return lax.ppermute(value, axis, [(i, i ^ bit) for i in range(lax.axis_size(axis))])


def summed_everywhere(value):
    for axis in ("rep", "fs", "tp"):
        size = lax.axis_size(axis)
        if size & (size - 1):
            value = lax.psum(value, axis)
            continue
        bit = 1
        while bit < size:
            value = value + swap(value, axis, bit)
            bit *= 2
    return value


def local(inputs, gain, gate_weight, up_weight, down_weight, cotangent):
    n_rep, n_tp = lax.axis_size("rep"), lax.axis_size("tp")
    if (n_rep, lax.axis_size("fs"), n_tp) == (2, N_Y * N_Z, 2):
        return fused(inputs, gain, gate_weight, up_weight, down_weight, cotangent)
    rep, tp = lax.axis_index("rep"), lax.axis_index("tp")
    rows, width = inputs.shape
    block = rows // n_tp
    units = gate_weight.shape[1] // n_rep

    def own_units(weight):
        return lax.dynamic_slice_in_dim(weight, rep * units, units, axis=1)

    def own_block(value, step):
        return lax.dynamic_slice_in_dim(value, (tp + step) % n_tp * block, block, axis=0)

    def gathered_tokens(value):
        parts = [own_block(value, s) for s in range(n_tp)]
        for j in range(1, n_rep):
            first = shift(own_block(value, 0), "rep", -j)
            parts += [first] + [shift(first, "tp", -s) for s in range(1, n_tp)]
        return jnp.concatenate(parts, axis=0)

    both_own = jnp.concatenate([own_units(gate_weight), own_units(up_weight)], axis=1)
    both_full = lax.all_gather(both_own, "fs", axis=0, tiled=True)
    down_full = lax.all_gather(own_units(down_weight), "fs", axis=0, tiled=True)
    tokens = gathered_tokens(inputs)
    cots = gathered_tokens(cotangent)

    def normed(value):
        single = value.astype(jnp.float32)
        inv = lax.rsqrt(jnp.mean(single * single, axis=-1, keepdims=True) + EPS)
        return single * inv, inv

    normalized_input = (normed(tokens)[0] * gain).astype(jnp.bfloat16)
    contract_cols = (((1,), (1,)), ((), ()))
    contract_rows = (((0,), (0,)), ((), ()))
    both = jnp.dot(normalized_input, both_full, preferred_element_type=jnp.float32)
    gate, up_proj = both[:, :units], both[:, units:]
    gate_sig = jax.nn.sigmoid(gate)
    active = gate * gate_sig
    hidden = (active * up_proj).astype(jnp.bfloat16)
    d_down_terms = (
        0.5 * lax.dot_general(cots, hidden, contract_rows, preferred_element_type=jnp.float32)
    ).astype(jnp.bfloat16)
    d_down_terms, cots = lax.optimization_barrier((d_down_terms, cots))
    summed = lax.psum_scatter(d_down_terms, "fs", scatter_dimension=0, tiled=True)
    d_hidden = 0.5 * jnp.dot(cots, down_full, preferred_element_type=jnp.float32)
    d_gate = (d_hidden * up_proj * gate_sig * (1.0 + gate * (1.0 - gate_sig))).astype(jnp.bfloat16)
    d_up = (d_hidden * active).astype(jnp.bfloat16)
    partial_value = (
        lax.dot_general(
            jnp.concatenate([d_gate, d_up], axis=1),
            both_full,
            contract_cols,
            preferred_element_type=jnp.float32,
        )
    ).astype(jnp.bfloat16).reshape(n_rep, n_tp, block, width)

    def tp_terms(step):
        return partial_value[:, step]

    over_tp = tp_terms(0).astype(jnp.float32)
    for s in range(1, n_tp):
        over_tp = over_tp + shift(tp_terms(s), "tp", s).astype(jnp.float32)
    over_tp = over_tp.astype(jnp.bfloat16)
    total = over_tp[0].astype(jnp.float32)
    for j in range(1, n_rep):
        total = total + shift(over_tp[j], "rep", j).astype(jnp.float32)
    normalized_gradient = total.astype(jnp.bfloat16).astype(jnp.float32)
    unit_input, inv = normed(own_block(inputs, 0))
    gain_gradient = summed_everywhere(jnp.sum(normalized_gradient * unit_input, axis=0))
    gain_scaled = gain * normalized_gradient
    mean_correction = jnp.mean(gain_scaled * unit_input, axis=-1, keepdims=True)
    block_gradient = (
        own_block(cotangent, 0).astype(jnp.float32)
        + inv * (gain_scaled - unit_input * mean_correction)
    ).astype(jnp.bfloat16)
    input_gradient = jnp.zeros((rows, width), jnp.bfloat16)
    for s in range(n_tp):
        piece = block_gradient if s == 0 else shift(block_gradient, "tp", -s)
        input_gradient = lax.dynamic_update_slice_in_dim(
            input_gradient, piece, (tp + s) % n_tp * block, axis=0
        )
    d_down = jnp.zeros((summed.shape[0], units * n_rep), jnp.float32)
    for j in range(n_rep):
        piece = summed if j == 0 else shift(summed, "rep", -j)
        d_down = lax.dynamic_update_slice_in_dim(
            d_down, piece.astype(jnp.float32), (rep + j) % n_rep * units, axis=1
        )
    return (input_gradient, gain_gradient, d_down)


def solution(mesh):
    placed = (
        P(("rep", "fs"), None),
        P(),
        P("fs", "tp"),
        P("fs", "tp"),
        P("fs", "tp"),
        P(("rep", "fs"), None),
    )
    return jax.shard_map(
        local,
        mesh=mesh,
        in_specs=placed,
        out_specs=(P(("rep", "fs"), None), P(), P("fs", "tp")),
        check_vma=False,
    )
```

```python
import jax
import jax.numpy as jnp
from jax import lax
from jax.experimental import pallas as pl
from jax.experimental.pallas import tpu as pltpu
from jax.sharding import PartitionSpec as P

EPS = 1e-06
F32, BF16 = jnp.float32, jnp.bfloat16
MESH_ID = pl.DeviceIdType.MESH
N_Y, N_Z = 2, 4
CHUNKS = 3
TOKEN_PARTS = 4
BACK_PARTS = 8


ORDER = ((0, 2, 1, 4, 3, 5, 6, 7, 8), (1, 3, 0, 2, 5, 4, 7, 6, 8))
Y_ORDER = tuple(
    tuple(("w", i) if isinstance(i, int) else ("t",) + i for i in order)
    for order in (
        (1, (0, 0), 3, (0, 1), 5, (0, 2), (0, 3), 7, 0, 2, (1, 0), (1, 1), (1, 2), (1, 3), 4, 6, 8),
        (0, 2, (0, 0), (0, 1), 4, (0, 2), (0, 3), 6, 1, (1, 0), 8, (1, 1), (1, 2), (1, 3), 3, 5, 7),
    )
)


SEND_GROUPS = {"yw": 0, "yt": 0, "ct": 0, "xw": 1, "up": 2, "dn": 3, "gc": 4, "gp": 4, "gz": 4}
LATE = 5
MERGED = {"xw": 2, "ct": 2, "ig": 1, "gp": 1, "gz": 1, "fx": 2}


def arrival(key):
    name = key[0]
    if name == "up":
        return ("zw", key[1], key[2], N_Z - key[3])
    if name == "dn":
        return ("zw",) + key[1:]
    if name == "rz":
        return ("rz", key[1], min(key[2] // 2, 1)) if key[2] > 2 else ("rz", key[1], 0)
    return key[: MERGED.get(name, len(key))]


def all_slots():
    keys = []
    for u in range(CHUNKS):
        keys.append(("xw", u))
        for w in range(3):
            keys.append(("yw", u, w))
            keys += [("zw", u, w, k) for k in range(1, N_Z)]
        if u:
            keys += [("rx", u, k) for k in range(N_Z)]
            keys += [("rz", u, 0), ("rz", u, 1), ("ry", u), ("fx", u)]
    keys += [("zh", i) for i in range(3)] + [("hx",), ("hy",)]
    for a in range(2):
        keys += [("yt", a, i) for i in range(TOKEN_PARTS)] + [("ct", a), ("cd", a)]
    keys += [("yd", i) for i in range(BACK_PARTS)]
    keys += [("ig",), ("gc",), ("gp",), ("gz",)]
    return {key: i for i, key in enumerate(keys)}


def fused_kernel(
    x, gain, gate_w, up_w, down_w, ct,
    ig, gg, dd,
    wgu, wd, xall, ctall, xn, inv, hid, dgu, dn, dd32, ddb, rx, zs, rz, fin, ry, fx,
    sd, rd, sy, yd, gp, gz, gvec, zh, zr, hx, hy,
    send, recv, own,
):
    slots = all_slots()
    rep, fs, tp = lax.axis_index("rep"), lax.axis_index("fs"), lax.axis_index("tp")
    z, y = fs // N_Y, fs % N_Y
    rows, width = x.shape
    wrows, cols = gate_w.shape
    units = cols // N_Y
    uc = units // CHUNKS
    half = rows // 2
    to_x, to_c = {"rep": 1 - rep}, {"tp": 1 - tp}
    to_y = {"fs": z * N_Y + 1 - y}
    to_xy = {"rep": 1 - rep, "fs": z * N_Y + 1 - y}
    to_up, to_dn = {"fs": fs + N_Y}, {"fs": fs - N_Y}
    z1 = z + 1 - 2 * (z % 2)
    z2 = (z + 2) % N_Z
    z3 = N_Z - 1 - z
    to_z = {1: {"fs": z1 * N_Y + y}, 2: {"fs": z2 * N_Y + y}, 3: {"fs": z3 * N_Y + y}}
    z_of = {1: z1, 2: z2, 3: z3}

    barrier = pltpu.get_barrier_semaphore()
    for target in (to_x, to_c, to_y, to_xy, to_z[1], to_z[2], to_z[3]):
        pl.semaphore_signal(barrier, inc=1, device_id=target, device_id_type=MESH_ID)
    pl.semaphore_wait(barrier, 7)

    def remote(key, src, dst, target):
        return pltpu.make_async_remote_copy(
            src_ref=src, dst_ref=dst,
            send_sem=send.at[SEND_GROUPS.get(key[0], LATE)],
            recv_sem=recv.at[slots[arrival(key)]],
            device_id=target, device_id_type=MESH_ID,
        )

    def start(key, src, dst, target):
        remote(key, src, dst, target).start()

    def wait(key, like):
        remote(key, like, like, to_x).wait_recv()

    tall = wrows * uc * 2 // (width * 4)

    def span(count):
        return dn.at[pl.ds(0, count * tall)]

    def sent(name, like):
        group = SEND_GROUPS.get(name, LATE)
        pltpu.make_async_remote_copy(
            src_ref=like, dst_ref=like, send_sem=send.at[group],
            recv_sem=recv.at[0], device_id=to_x, device_id_type=MESH_ID,
        ).wait_send()

    def region(u, w, owner):
        r = pl.ds(pl.multiple_of(owner * wrows, wrows), wrows)
        if w == 2:
            return wd.at[u, r]
        return wgu.at[u, r, pl.ds(w * uc, uc)]

    weights = (gate_w, up_w, down_w)

    def part(w, who, u):
        return weights[w].at[:, pl.ds(pl.multiple_of(who * units + u * uc, uc), uc)]

    def y_weights(u, w):
        start(("yw", u, w), part(w, 1 - y, u), region(u, w, fs), to_y)

    own_tokens = pl.multiple_of(y * rows, rows)
    other_tokens = pl.multiple_of((1 - y) * rows, rows)
    tpart = half // TOKEN_PARTS

    def y_tokens(a, i):
        full = (xall, ctall)[a]
        r = pl.ds(pl.multiple_of(own_tokens + tp * half + i * tpart, tpart), tpart)
        start(("yt", a, i), full.at[r], full.at[r], to_y)

    def core_tokens(a, i):
        full = (xall, ctall)[a]
        r = pl.ds(pl.multiple_of(other_tokens + tp * half + i * tpart, tpart), tpart)
        wait(("yt", a, i), full.at[r])
        start(("ct", a, i), full.at[r], full.at[r], to_c)

    pieces = [(u, w) for u in range(CHUNKS) for w in range(3)]

    def local_copy(n):
        u, w = pieces[n]
        return pltpu.make_async_copy(part(w, y, u), region(u, w, fs), own.at[2 + n])

    kept = [local_copy(n) for n in range(len(pieces))]
    kept_tokens = [
        pltpu.make_async_copy(source, full.at[pl.ds(own_tokens, rows)], own.at[a])
        for a, (source, full) in enumerate(((x, xall), (ct, ctall)))
    ]

    def each_rep(step):
        for r in range(2):

            @pl.when(rep == r)
            def _():
                step(r)

    def y_step(r, item):
        if item[0] == "w":
            y_weights(*pieces[item[1]])
        else:
            y_tokens(item[1], item[2])

    def carried(n, r, owner):
        return owner * N_Y + (y if (r + n) % 2 == 0 else 1 - y)

    def own_send(slot):
        def step(r):
            n = ORDER[r][slot]
            u, w = pieces[n]
            if (r + n) % 2:
                wait(("yw", u, w), region(u, w, fs))
            src = region(u, w, carried(n, r, z))

            @pl.when(z < N_Z - 1)
            def _():
                start(("up", u, w, 1), src, src, to_up)

            @pl.when(z > 0)
            def _():
                start(("dn", u, w, 1), src, src, to_dn)

        each_rep(step)

    def arrive(slot, d):
        def step(r):
            n = ORDER[r][slot]
            u, w = pieces[n]

            @pl.when(z - d >= 0)
            def _():
                src = region(u, w, carried(n, r, z - d))
                wait(("up", u, w, d), src)
                if d < N_Z - 1:

                    @pl.when(z < N_Z - 1)
                    def _():
                        start(("up", u, w, d + 1), src, src, to_up)

                start(("xw", u, w, N_Z - d), src, src, to_x)

            @pl.when(z + d <= N_Z - 1)
            def _():
                src = region(u, w, carried(n, r, z + d))
                wait(("dn", u, w, d), src)
                if d < N_Z - 1:

                    @pl.when(z > 0)
                    def _():
                        start(("dn", u, w, d + 1), src, src, to_dn)

                start(("xw", u, w, d), src, src, to_x)

        each_rep(step)

    def chunk_ready(u):
        for w in range(3):
            n = pieces.index((u, w))
            like = region(u, w, fs)

            @pl.when(rep == n % 2)
            def _():
                wait(("yw", u, w), like)

        wait(("xw", u), span(3 * (N_Z - 1)))

    gain_row = gain[...]
    norm_rows = 64

    def normalize(first):
        def body(i, _):
            r = pl.ds(pl.multiple_of(first + i * norm_rows, norm_rows), norm_rows)
            single = xall[r, :].astype(F32)
            scale = lax.rsqrt(jnp.mean(single * single, axis=-1, keepdims=True) + EPS)
            inv[r, :] = scale
            xn[r, :] = (single * scale * gain_row).astype(BF16)
            return 0

        lax.fori_loop(0, rows // norm_rows, body, 0)

    def forward(u, first):
        r = pl.ds(first, rows)
        both = jnp.dot(xn[r, :], wgu[u], preferred_element_type=F32)
        gate, up = both[:, :uc], both[:, uc:]
        sig = jax.nn.sigmoid(gate)
        active = gate * sig
        hid[u, r, :] = (active * up).astype(BF16)
        d_hidden = 0.5 * jnp.dot(ctall[r, :], wd[u], preferred_element_type=F32)
        dgu[u, r, :uc] = (d_hidden * up * sig * (1.0 + gate * (1.0 - sig))).astype(BF16)
        dgu[u, r, uc:] = (d_hidden * active).astype(BF16)

    over_rows = (((0,), (0,)), ((), ()))
    over_cols = (((1,), (1,)), ((), ()))

    def down_terms(u):
        def body(zd, _):
            r = pl.ds(pl.multiple_of(zd * 2 * wrows, 2 * wrows), 2 * wrows)
            value = 0.5 * lax.dot_general(
                ctall[:, r], hid[u], over_rows, preferred_element_type=F32
            )
            dd32[u, zd] = value.reshape(2, 2, wrows // 2, uc)
            if u:
                ddb[u - 1, zd] = dd32[u, zd, :, 1 - rep].astype(BF16)
            return 0

        lax.fori_loop(0, N_Z, body, 0)

    def put(u, side, who, value):
        r = pl.ds(pl.multiple_of(side * (wrows // 2), wrows // 2), wrows // 2)
        c = pl.ds(pl.multiple_of(who * units + u * uc, uc), uc)
        dd[r, c] = value.astype(F32)

    def first_to_z():
        zh[1] = dd32[0, z3].astype(BF16)
        start(("zh", 1), zh.at[1], zr.at[1], to_z[1])
        zh[0] = dd32[0, z1].astype(BF16)
        start(("zh", 0), zh.at[0], zr.at[0], to_z[1])

    def first_on_z():
        wait(("zh", 1), zr.at[1])
        zh[2] = (dd32[0, z2] + zr[1].astype(F32)).astype(BF16)
        start(("zh", 2), zh.at[2], zr.at[2], to_z[2])

    def first_to_x():
        wait(("zh", 0), zr.at[0])
        wait(("zh", 2), zr.at[2])
        total = dd32[0, z] + zr[0].astype(F32) + zr[2].astype(F32)
        hx[0] = total.astype(BF16)
        start(("hx",), hx.at[0], hx.at[1], to_x)

    def first_to_y():
        wait(("hx",), hx.at[1])
        total = (hx[0].astype(F32) + hx[1].astype(F32)).astype(BF16)
        zr[0] = total
        hy[0] = zr[0, 1 - y]
        start(("hy",), hy.at[0], hy.at[1], to_y)
        for side in range(2):
            put(0, side, y, zr[0, y, side])

    def first_final():
        wait(("hy",), hy.at[1])
        for side in range(2):
            put(0, side, 1 - y, hy[1, side])

    def down_to_x(u, ks=(3, 2, 1, 0)):
        for k in ks:
            zd = z if k == 0 else z_of[k]
            start(("rx", u, k), ddb.at[u - 1, zd], rx.at[u - 1, zd], to_x)

    def down_along_z(u, k):
        zd = z if k == 0 else z_of[k]
        wait(("rx", u, k), rx.at[u - 1, zd])
        total = dd32[u, zd, :, rep] + rx[u - 1, zd].astype(F32)
        if k == 0:
            fin[u - 1] = total
            return
        if k == 2:
            wait(("rz", u, 3), rz.at[u - 1, 3])
            total = total + rz[u - 1, 3].astype(F32)
        zs[u - 1, k] = total.astype(BF16)
        start(("rz", u, k), zs.at[u - 1, k], rz.at[u - 1, k], to_z[2 if k == 2 else 1])

    def down_final(u):
        total = fin[u - 1]
        wait(("rz", u, 1), rz.at[u - 1, pl.ds(1, 2)])
        for k in (1, 2):
            total = total + rz[u - 1, k].astype(F32)
        zs[u - 1, 0] = total.astype(BF16)
        start(("ry", u), zs.at[u - 1, 0, 1 - y], ry.at[u - 1], to_y)
        if u == CHUNKS - 1:
            start(("fx", u, 1), zs.at[u - 1, 0, 1 - y], fx.at[u - 1, 1], to_xy)
        start(("fx", u, 0), zs.at[u - 1, 0, y], fx.at[u - 1, 0], to_x)
        put(u, rep, y, zs[u - 1, 0, y])

    def down_y(u):
        wait(("ry", u), ry.at[u - 1])
        if u < CHUNKS - 1:
            start(("fx", u, 1), ry.at[u - 1], fx.at[u - 1, 1], to_x)
        put(u, rep, 1 - y, ry[u - 1])

    def down_x(u):
        wait(("fx", u), fx.at[u - 1])
        put(u, 1 - rep, y, fx[u - 1, 0])
        put(u, 1 - rep, 1 - y, fx[u - 1, 1])

    n_cols = 512

    def back(first, chunks, add=False):
        def body(j, _):
            c = pl.ds(pl.multiple_of(j * n_cols, n_cols), n_cols)
            total = dn[pl.ds(first, half), c] if add else None
            for u in chunks:
                term = lax.dot_general(
                    dgu[u, pl.ds(first, half), :], wgu[u, c, :], over_cols,
                    preferred_element_type=F32,
                )
                total = term if total is None else total + term
            dn[pl.ds(first, half), c] = total
            return 0

        lax.fori_loop(0, width // n_cols, body, 0)

    def back_to_core(h, first):
        r = pl.ds(pl.multiple_of(first + (1 - tp) * half, half), half)
        sd[h] = dn[r, :].astype(BF16)
        start(("cd", h), sd.at[h], rd.at[h], to_c)

    def half_of(first, who):
        return pl.multiple_of(first + who * half, half)

    bpart = half // BACK_PARTS

    def back_to_y(i):
        if i == 0:
            wait(("cd", 0), rd.at[0])
        r = pl.ds(pl.multiple_of(other_tokens + tp * half + i * bpart, bpart), bpart)
        q = pl.ds(i * bpart, bpart)
        mine = dn[r, :].astype(BF16).astype(F32)
        sy[q, :] = (mine + rd[0, q, :].astype(F32)).astype(BF16)
        start(("yd", i), sy.at[q], yd.at[q], to_y)

    def gain_terms(first):
        def body(i, acc):
            r = pl.ds(pl.multiple_of(first + i * norm_rows, norm_rows), norm_rows)
            terms = dn[r, :] * (xall[r, :].astype(F32) * inv[r, :])
            return acc + jnp.sum(terms.reshape(norm_rows // 8, 8, width), axis=0)

        return lax.fori_loop(0, rows // norm_rows, body, jnp.zeros((8, width), F32))

    in_plane = rep * N_Y + y

    def gain_core():
        acc = gain_terms(own_tokens) + gain_terms(other_tokens)
        gvec[0] = jnp.sum(acc, axis=0, keepdims=True)
        start(("gc",), gvec.at[0], gvec.at[1], to_c)

    def gain_plane():
        wait(("gc",), gvec.at[1])
        gp[in_plane] = gvec[0] + gvec[1]
        here = gp.at[in_plane]
        for i, target in enumerate((to_y, to_x, to_xy)):
            start(("gp", i), here, here, target)

    def gain_z():
        wait(("gp",), gp.at[pl.ds(0, 3)])
        gz[z] = gp[0] + gp[1] + gp[2] + gp[3]
        for i in range(3):
            start(("gz", i), gz.at[z], gz.at[z], to_z[i + 1])

    def gain_end():
        wait(("gz",), gz.at[pl.ds(0, 3)])
        gg[...] = gz[0] + gz[1] + gz[2] + gz[3]

    out_row = pl.multiple_of(tp * half, half)

    def back_final(i):
        q = pl.ds(i * bpart, bpart)
        wait(("yd", i), yd.at[q])
        r = pl.ds(pl.multiple_of(own_tokens + tp * half + i * bpart, bpart), bpart)
        mine = dn[r, :].astype(BF16).astype(F32) + rd[1, q, :].astype(F32)
        mine = mine.astype(BF16).astype(F32) + yd[q, :].astype(F32)
        mine = mine.astype(BF16).astype(F32)
        scale = inv[r, :]
        unit = xall[r, :].astype(F32) * scale
        scaled = gain_row * mine
        mean = jnp.mean(scaled * unit, axis=-1, keepdims=True)
        o = pl.ds(pl.multiple_of(out_row + i * bpart, bpart), bpart)
        ig[o, :] = (ctall[r, :].astype(F32) + scale * (scaled - unit * mean)).astype(BF16)
        start(("ig", i), ig.at[o], ig.at[o], to_c)

    def gather_sent():
        sent("yw", span(3 * CHUNKS + 2 * TOKEN_PARTS * 2 * 2))
        sent("xw", span(3 * CHUNKS * (N_Z - 1)))
        for i in range(N_Z - 1):

            @pl.when(z == i)
            def _():
                sent("up", span(3 * CHUNKS * (i + 1)))

            @pl.when(z == N_Z - 1 - i)
            def _():
                sent("dn", span(3 * CHUNKS * (i + 1)))

    def y_upto(limit):
        def step(r):
            spent = 0
            for item in Y_ORDER[r]:
                cost = 1 if item[0] == "w" else 2
                if y_done[0] <= spent < limit:
                    y_step(r, item)
                spent += cost

        each_rep(step)
        y_done[0] = limit

    def core_token_group(a, parts):
        for i in parts:
            core_tokens(a, i)

    def tokens_ready(a):
        wait(("ct", a), (xall, ctall)[a].at[pl.ds(0, half)])

    y_done = [0]
    y_upto(1)
    for n in (0, 1, 2, 3):
        kept[n].start()
    kept_tokens[0].start()
    for n in range(4, len(pieces)):
        kept[n].start()
    kept_tokens[1].start()
    for n in (0, 1):
        kept[n].wait()
    own_send(0)
    kept_tokens[0].wait()
    y_upto(4)
    normalize(own_tokens)
    for copy in kept[2:] + kept_tokens[1:]:
        copy.wait()
    own_send(1)
    last = len(pieces)
    for t in range(last + 2):
        y_upto(3 * t + 7)
        if t + 2 < last and t + 2 >= 3:
            own_send(t + 2)
        for d in range(1, N_Z):
            if t == 8 and d == 3:
                tokens_ready(1)
                forward(0, other_tokens)
            if t == 9 and d == 3:
                first_to_z()
                chunk_ready(1)
                forward(1, own_tokens)
            if 0 <= t + 1 - d < last:
                arrive(t + 1 - d, d)
            if t == 0 and d == 1:
                own_send(2)
        if t == 2:
            core_token_group(0, (0, 1))
        if t == 4:
            core_token_group(0, (2, 3))
        if t == 5:
            tokens_ready(0)
            normalize(other_tokens)
        if t == 6:
            core_token_group(1, (0, 1))
            chunk_ready(0)
            forward(0, own_tokens)
        if t == 7:
            core_token_group(1, (2, 3))
        if t == 8:
            down_terms(0)
    forward(1, other_tokens)
    down_terms(1)
    down_to_x(1)
    early = tuple(range(CHUNKS - 1))
    final = CHUNKS - 1
    back(half_of(other_tokens, 1 - tp), early)
    back(half_of(other_tokens, tp), early)
    chunk_ready(final)
    forward(final, other_tokens)
    back(half_of(other_tokens, 1 - tp), (final,), True)
    back_to_core(0, other_tokens)
    first_on_z()
    down_along_z(1, 3)
    back(half_of(other_tokens, tp), (final,), True)
    for i in range(BACK_PARTS - 2):
        back_to_y(i)
    forward(2, own_tokens)
    down_along_z(1, 1)
    down_terms(2)
    down_to_x(2)
    back(half_of(own_tokens, 1 - tp), range(CHUNKS))
    back_to_core(1, own_tokens)
    down_along_z(1, 2)
    down_along_z(1, 0)
    back(half_of(own_tokens, tp), range(CHUNKS))
    gain_core()
    down_along_z(2, 3)
    gain_plane()
    for i in range(BACK_PARTS - 2, BACK_PARTS):
        back_to_y(i)
    first_to_x()
    wait(("cd", 1), rd.at[1])
    down_along_z(2, 1)
    down_final(1)
    back_final(0)
    back_final(1)
    down_along_z(2, 2)
    down_along_z(2, 0)
    gather_sent()
    gain_z()
    back_final(2)
    back_final(3)
    back_final(4)
    back_final(5)
    first_to_y()
    down_final(2)
    down_y(1)
    back_final(6)
    back_final(7)
    down_x(1)
    gain_end()
    first_final()
    down_y(2)
    down_x(2)
    wait(("ig",), ig.at[pl.ds(0, half)])
    rest = (CHUNKS - 1) * (N_Z + N_Z - 1) + 3 * (CHUNKS - 1) // 2 + 3 * 2 + 2 + 1
    moved = 2 * half * width // (wrows * uc)
    sent("late", span(rest + 2 * moved))
    sent("gc", gp.at[pl.ds(0, 7)])

def fused(x, gain, gate_w, up_w, down_w, ct):
    rows, width = x.shape
    wrows, cols = gate_w.shape
    units = cols // N_Y
    uc = units // CHUNKS
    half = rows // 2
    n = len(all_slots())
    vm = pltpu.VMEM
    anywhere = pl.BlockSpec(memory_space=pl.ANY)
    tile = (2, wrows // 2, uc)
    ig, gg, dd = pl.pallas_call(
        fused_kernel,
        out_shape=[
            vm((rows, width), BF16),
            vm((1, width), F32),
            vm((wrows, cols), F32),
        ],
        in_specs=[anywhere, pl.BlockSpec(memory_space=vm)] + [anywhere] * 4,
        out_specs=[pl.BlockSpec(memory_space=vm)] * 3,
        scratch_shapes=[
            vm((CHUNKS, width, 2 * uc), BF16),
            vm((CHUNKS, width, uc), BF16),
            vm((2 * rows, width), BF16),
            vm((2 * rows, width), BF16),
            vm((2 * rows, width), BF16),
            vm((2 * rows, 1), F32),
            vm((CHUNKS, 2 * rows, uc), BF16),
            vm((CHUNKS, 2 * rows, 2 * uc), BF16),
            vm((2 * rows, width), F32),
            vm((CHUNKS, N_Z, 2) + tile, F32),
            vm((CHUNKS - 1, N_Z) + tile, BF16),
            vm((CHUNKS - 1, N_Z) + tile, BF16),
            vm((CHUNKS - 1, N_Z) + tile, BF16),
            vm((CHUNKS - 1, N_Z) + tile, BF16),
            vm((CHUNKS - 1,) + tile, F32),
            vm((CHUNKS - 1,) + tile[1:], BF16),
            vm((CHUNKS - 1,) + tile, BF16),
            vm((2, half, width), BF16),
            vm((2, half, width), BF16),
            vm((half, width), BF16),
            vm((half, width), BF16),
            vm((8, 1, width), F32),
            vm((N_Z, 1, width), F32),
            vm((2, 1, width), F32),
            vm((3, 2) + tile, BF16),
            vm((3, 2) + tile, BF16),
            vm((2, 2) + tile, BF16),
            vm((2,) + tile, BF16),
            pltpu.SemaphoreType.DMA((LATE + 1,)),
            pltpu.SemaphoreType.DMA((n,)),
            pltpu.SemaphoreType.DMA((2 + 3 * CHUNKS,)),
        ],
        compiler_params=pltpu.CompilerParams(
            collective_id=0, has_side_effects=True, vmem_limit_bytes=62500000
        ),
        name="fused",
    )(x, gain.reshape(1, width), gate_w, up_w, down_w, ct)
    return ig, gg.reshape(width), dd


def shift(value, axis, step):
    size = lax.axis_size(axis)
    return lax.ppermute(value, axis, [(i, (i + step) % size) for i in range(size)])


def swap(value, axis, bit):
    return lax.ppermute(value, axis, [(i, i ^ bit) for i in range(lax.axis_size(axis))])


def summed_everywhere(value):
    for axis in ("rep", "fs", "tp"):
        size = lax.axis_size(axis)
        if size & (size - 1):
            value = lax.psum(value, axis)
            continue
        bit = 1
        while bit < size:
            value = value + swap(value, axis, bit)
            bit *= 2
    return value


def local(inputs, gain, gate_weight, up_weight, down_weight, cotangent):
    n_rep, n_tp = lax.axis_size("rep"), lax.axis_size("tp")
    if (n_rep, lax.axis_size("fs"), n_tp) == (2, N_Y * N_Z, 2):
        return fused(inputs, gain, gate_weight, up_weight, down_weight, cotangent)
    rep, tp = lax.axis_index("rep"), lax.axis_index("tp")
    rows, width = inputs.shape
    block = rows // n_tp
    units = gate_weight.shape[1] // n_rep

    def own_units(weight):
        return lax.dynamic_slice_in_dim(weight, rep * units, units, axis=1)

    def own_block(value, step):
        return lax.dynamic_slice_in_dim(value, (tp + step) % n_tp * block, block, axis=0)

    def gathered_tokens(value):
        parts = [own_block(value, s) for s in range(n_tp)]
        for j in range(1, n_rep):
            first = shift(own_block(value, 0), "rep", -j)
            parts += [first] + [shift(first, "tp", -s) for s in range(1, n_tp)]
        return jnp.concatenate(parts, axis=0)

    both_own = jnp.concatenate([own_units(gate_weight), own_units(up_weight)], axis=1)
    both_full = lax.all_gather(both_own, "fs", axis=0, tiled=True)
    down_full = lax.all_gather(own_units(down_weight), "fs", axis=0, tiled=True)
    tokens = gathered_tokens(inputs)
    cots = gathered_tokens(cotangent)

    def normed(value):
        single = value.astype(jnp.float32)
        inv = lax.rsqrt(jnp.mean(single * single, axis=-1, keepdims=True) + EPS)
        return single * inv, inv

    normalized_input = (normed(tokens)[0] * gain).astype(jnp.bfloat16)
    contract_cols = (((1,), (1,)), ((), ()))
    contract_rows = (((0,), (0,)), ((), ()))
    both = jnp.dot(normalized_input, both_full, preferred_element_type=jnp.float32)
    gate, up_proj = both[:, :units], both[:, units:]
    gate_sig = jax.nn.sigmoid(gate)
    active = gate * gate_sig
    hidden = (active * up_proj).astype(jnp.bfloat16)
    d_down_terms = (
        0.5 * lax.dot_general(cots, hidden, contract_rows, preferred_element_type=jnp.float32)
    ).astype(jnp.bfloat16)
    d_down_terms, cots = lax.optimization_barrier((d_down_terms, cots))
    summed = lax.psum_scatter(d_down_terms, "fs", scatter_dimension=0, tiled=True)
    d_hidden = 0.5 * jnp.dot(cots, down_full, preferred_element_type=jnp.float32)
    d_gate = (d_hidden * up_proj * gate_sig * (1.0 + gate * (1.0 - gate_sig))).astype(jnp.bfloat16)
    d_up = (d_hidden * active).astype(jnp.bfloat16)
    partial_value = (
        lax.dot_general(
            jnp.concatenate([d_gate, d_up], axis=1),
            both_full,
            contract_cols,
            preferred_element_type=jnp.float32,
        )
    ).astype(jnp.bfloat16).reshape(n_rep, n_tp, block, width)

    def tp_terms(step):
        return partial_value[:, step]

    over_tp = tp_terms(0).astype(jnp.float32)
    for s in range(1, n_tp):
        over_tp = over_tp + shift(tp_terms(s), "tp", s).astype(jnp.float32)
    over_tp = over_tp.astype(jnp.bfloat16)
    total = over_tp[0].astype(jnp.float32)
    for j in range(1, n_rep):
        total = total + shift(over_tp[j], "rep", j).astype(jnp.float32)
    normalized_gradient = total.astype(jnp.bfloat16).astype(jnp.float32)
    unit_input, inv = normed(own_block(inputs, 0))
    gain_gradient = summed_everywhere(jnp.sum(normalized_gradient * unit_input, axis=0))
    gain_scaled = gain * normalized_gradient
    mean_correction = jnp.mean(gain_scaled * unit_input, axis=-1, keepdims=True)
    block_gradient = (
        own_block(cotangent, 0).astype(jnp.float32)
        + inv * (gain_scaled - unit_input * mean_correction)
    ).astype(jnp.bfloat16)
    input_gradient = jnp.zeros((rows, width), jnp.bfloat16)
    for s in range(n_tp):
        piece = block_gradient if s == 0 else shift(block_gradient, "tp", -s)
        input_gradient = lax.dynamic_update_slice_in_dim(
            input_gradient, piece, (tp + s) % n_tp * block, axis=0
        )
    d_down = jnp.zeros((summed.shape[0], units * n_rep), jnp.float32)
    for j in range(n_rep):
        piece = summed if j == 0 else shift(summed, "rep", -j)
        d_down = lax.dynamic_update_slice_in_dim(
            d_down, piece.astype(jnp.float32), (rep + j) % n_rep * units, axis=1
        )
    return (input_gradient, gain_gradient, d_down)


def solution(mesh):
    placed = (
        P(("rep", "fs"), None),
        P(),
        P("fs", "tp"),
        P("fs", "tp"),
        P("fs", "tp"),
        P(("rep", "fs"), None),
    )
    return jax.shard_map(
        local,
        mesh=mesh,
        in_specs=placed,
        out_specs=(P(("rep", "fs"), None), P(), P("fs", "tp")),
        check_vma=False,
    )
```

```python
import jax
import jax.numpy as jnp
from jax import lax
from jax.experimental import pallas as pl
from jax.experimental.pallas import tpu as pltpu
from jax.sharding import PartitionSpec as P

EPS = 1e-06
F32, BF16 = jnp.float32, jnp.bfloat16
MESH_ID = pl.DeviceIdType.MESH
N_Y, N_Z = 2, 4
CHUNKS = 3
TOKEN_PARTS = 4
BACK_PARTS = 8


ORDER = ((0, 2, 1, 4, 3, 5, 6, 7, 8), (1, 3, 0, 2, 5, 4, 7, 6, 8))
Y_ORDER = tuple(
    tuple(("w", i) if isinstance(i, int) else ("t",) + i for i in order)
    for order in (
        (1, (0, 0), 3, (0, 1), 5, (0, 2), (0, 3), 7, 0, 2, (1, 0), (1, 1), (1, 2), (1, 3), 4, 6, 8),
        (0, 2, (0, 0), (0, 1), 4, (0, 2), (0, 3), 6, 1, (1, 0), 8, (1, 1), (1, 2), (1, 3), 3, 5, 7),
    )
)


SEND_GROUPS = {"yw": 0, "yt": 0, "ct": 0, "xw": 1, "up": 2, "dn": 3, "gc": 4, "gp": 4, "gz": 4}
LATE = 5
MERGED = {"xw": 2, "ct": 2, "ig": 1, "gp": 1, "gz": 1, "fx": 2}


def arrival(key):
    name = key[0]
    if name == "up":
        return ("zw", key[1], key[2], N_Z - key[3])
    if name == "dn":
        return ("zw",) + key[1:]
    if name == "rz":
        return ("rz", key[1], min(key[2] // 2, 1)) if key[2] > 2 else ("rz", key[1], 0)
    return key[: MERGED.get(name, len(key))]


def all_slots():
    keys = []
    for u in range(CHUNKS):
        keys.append(("xw", u))
        for w in range(3):
            keys.append(("yw", u, w))
            keys += [("zw", u, w, k) for k in range(1, N_Z)]
        if u:
            keys += [("rx", u, k) for k in range(N_Z)]
            keys += [("rz", u, 0), ("rz", u, 1), ("ry", u), ("fx", u)]
    keys += [("zh", i) for i in range(3)] + [("hx",), ("hy",)]
    for a in range(2):
        keys += [("yt", a, i) for i in range(TOKEN_PARTS)] + [("ct", a), ("cd", a)]
    keys += [("yd", i) for i in range(BACK_PARTS)]
    keys += [("ig",), ("gc",), ("gp",), ("gz",)]
    return {key: i for i, key in enumerate(keys)}


def fused_kernel(
    x, gain, gate_w, up_w, down_w, ct,
    ig, gg, dd,
    wgu, wd, xall, ctall, xn, inv, hid, dgu, dn, dd32, ddb, rx, zs, rz, fin, ry, fx,
    sd, rd, sy, yd, gp, gz, gvec, zh, zr, hx, hy,
    send, recv, own,
):
    slots = all_slots()
    rep, fs, tp = lax.axis_index("rep"), lax.axis_index("fs"), lax.axis_index("tp")
    z, y = fs // N_Y, fs % N_Y
    rows, width = x.shape
    wrows, cols = gate_w.shape
    units = cols // N_Y
    uc = units // CHUNKS
    half = rows // 2
    to_x, to_c = {"rep": 1 - rep}, {"tp": 1 - tp}
    to_y = {"fs": z * N_Y + 1 - y}
    to_xy = {"rep": 1 - rep, "fs": z * N_Y + 1 - y}
    to_up, to_dn = {"fs": fs + N_Y}, {"fs": fs - N_Y}
    z1 = z + 1 - 2 * (z % 2)
    z2 = (z + 2) % N_Z
    z3 = N_Z - 1 - z
    to_z = {1: {"fs": z1 * N_Y + y}, 2: {"fs": z2 * N_Y + y}, 3: {"fs": z3 * N_Y + y}}
    z_of = {1: z1, 2: z2, 3: z3}

    barrier = pltpu.get_barrier_semaphore()
    for target in (to_x, to_c, to_y, to_xy, to_z[1], to_z[2], to_z[3]):
        pl.semaphore_signal(barrier, inc=1, device_id=target, device_id_type=MESH_ID)
    pl.semaphore_wait(barrier, 7)

    def remote(key, src, dst, target):
        return pltpu.make_async_remote_copy(
            src_ref=src, dst_ref=dst,
            send_sem=send.at[SEND_GROUPS.get(key[0], LATE)],
            recv_sem=recv.at[slots[arrival(key)]],
            device_id=target, device_id_type=MESH_ID,
        )

    def start(key, src, dst, target):
        remote(key, src, dst, target).start()

    def wait(key, like):
        remote(key, like, like, to_x).wait_recv()

    tall = wrows * uc * 2 // (width * 4)

    def span(count):
        return dn.at[pl.ds(0, count * tall)]

    def sent(name, like):
        group = SEND_GROUPS.get(name, LATE)
        pltpu.make_async_remote_copy(
            src_ref=like, dst_ref=like, send_sem=send.at[group],
            recv_sem=recv.at[0], device_id=to_x, device_id_type=MESH_ID,
        ).wait_send()

    def region(u, w, owner):
        r = pl.ds(pl.multiple_of(owner * wrows, wrows), wrows)
        if w == 2:
            return wd.at[u, r]
        return wgu.at[u, r, pl.ds(w * uc, uc)]

    weights = (gate_w, up_w, down_w)

    def part(w, who, u):
        return weights[w].at[:, pl.ds(pl.multiple_of(who * units + u * uc, uc), uc)]

    def y_weights(u, w):
        start(("yw", u, w), part(w, 1 - y, u), region(u, w, fs), to_y)

    own_tokens = pl.multiple_of(y * rows, rows)
    other_tokens = pl.multiple_of((1 - y) * rows, rows)
    tpart = half // TOKEN_PARTS

    def y_tokens(a, i):
        full = (xall, ctall)[a]
        r = pl.ds(pl.multiple_of(own_tokens + tp * half + i * tpart, tpart), tpart)
        start(("yt", a, i), full.at[r], full.at[r], to_y)

    def core_tokens(a, i):
        full = (xall, ctall)[a]
        r = pl.ds(pl.multiple_of(other_tokens + tp * half + i * tpart, tpart), tpart)
        wait(("yt", a, i), full.at[r])
        start(("ct", a, i), full.at[r], full.at[r], to_c)

    pieces = [(u, w) for u in range(CHUNKS) for w in range(3)]

    def local_copy(n):
        u, w = pieces[n]
        return pltpu.make_async_copy(part(w, y, u), region(u, w, fs), own.at[2 + n])

    kept = [local_copy(n) for n in range(len(pieces))]
    kept_tokens = [
        pltpu.make_async_copy(source, full.at[pl.ds(own_tokens, rows)], own.at[a])
        for a, (source, full) in enumerate(((x, xall), (ct, ctall)))
    ]

    def each_rep(step):
        for r in range(2):

            @pl.when(rep == r)
            def _():
                step(r)

    def y_step(r, item):
        if item[0] == "w":
            y_weights(*pieces[item[1]])
        else:
            y_tokens(item[1], item[2])

    def carried(n, r, owner):
        return owner * N_Y + (y if (r + n) % 2 == 0 else 1 - y)

    def own_send(slot):
        def step(r):
            n = ORDER[r][slot]
            u, w = pieces[n]
            if (r + n) % 2:
                wait(("yw", u, w), region(u, w, fs))
            src = region(u, w, carried(n, r, z))

            @pl.when(z < N_Z - 1)
            def _():
                start(("up", u, w, 1), src, src, to_up)

            @pl.when(z > 0)
            def _():
                start(("dn", u, w, 1), src, src, to_dn)

        each_rep(step)

    def arrive(slot, d):
        def step(r):
            n = ORDER[r][slot]
            u, w = pieces[n]

            @pl.when(z - d >= 0)
            def _():
                src = region(u, w, carried(n, r, z - d))
                wait(("up", u, w, d), src)
                if d < N_Z - 1:

                    @pl.when(z < N_Z - 1)
                    def _():
                        start(("up", u, w, d + 1), src, src, to_up)

                start(("xw", u, w, N_Z - d), src, src, to_x)

            @pl.when(z + d <= N_Z - 1)
            def _():
                src = region(u, w, carried(n, r, z + d))
                wait(("dn", u, w, d), src)
                if d < N_Z - 1:

                    @pl.when(z > 0)
                    def _():
                        start(("dn", u, w, d + 1), src, src, to_dn)

                start(("xw", u, w, d), src, src, to_x)

        each_rep(step)

    def chunk_ready(u):
        for w in range(3):
            n = pieces.index((u, w))
            like = region(u, w, fs)

            @pl.when(rep == n % 2)
            def _():
                wait(("yw", u, w), like)

        wait(("xw", u), span(3 * (N_Z - 1)))

    gain_row = gain[...]
    norm_rows = 64

    def normalize(first):
        def body(i, _):
            r = pl.ds(pl.multiple_of(first + i * norm_rows, norm_rows), norm_rows)
            single = xall[r, :].astype(F32)
            scale = lax.rsqrt(jnp.mean(single * single, axis=-1, keepdims=True) + EPS)
            inv[r, :] = scale
            xn[r, :] = (single * scale * gain_row).astype(BF16)
            return 0

        lax.fori_loop(0, rows // norm_rows, body, 0)

    def forward(u, first):
        r = pl.ds(first, rows)
        both = jnp.dot(xn[r, :], wgu[u], preferred_element_type=F32)
        gate, up = both[:, :uc], both[:, uc:]
        sig = jax.nn.sigmoid(gate)
        active = gate * sig
        hid[u, r, :] = (active * up).astype(BF16)
        d_hidden = 0.5 * jnp.dot(ctall[r, :], wd[u], preferred_element_type=F32)
        dgu[u, r, :uc] = (d_hidden * up * sig * (1.0 + gate * (1.0 - sig))).astype(BF16)
        dgu[u, r, uc:] = (d_hidden * active).astype(BF16)

    over_rows = (((0,), (0,)), ((), ()))
    over_cols = (((1,), (1,)), ((), ()))

    def down_terms(u):
        def body(zd, _):
            r = pl.ds(pl.multiple_of(zd * 2 * wrows, 2 * wrows), 2 * wrows)
            value = 0.5 * lax.dot_general(
                ctall[:, r], hid[u], over_rows, preferred_element_type=F32
            )
            dd32[u, zd] = value.reshape(2, 2, wrows // 2, uc)
            if u:
                ddb[u - 1, zd] = dd32[u, zd, :, 1 - rep].astype(BF16)
            return 0

        lax.fori_loop(0, N_Z, body, 0)

    def put(u, side, who, value):
        r = pl.ds(pl.multiple_of(side * (wrows // 2), wrows // 2), wrows // 2)
        c = pl.ds(pl.multiple_of(who * units + u * uc, uc), uc)
        dd[r, c] = value.astype(F32)

    def first_to_z():
        zh[1] = dd32[0, z3].astype(BF16)
        start(("zh", 1), zh.at[1], zr.at[1], to_z[1])
        zh[0] = dd32[0, z1].astype(BF16)
        start(("zh", 0), zh.at[0], zr.at[0], to_z[1])

    def first_on_z():
        wait(("zh", 1), zr.at[1])
        zh[2] = (dd32[0, z2] + zr[1].astype(F32)).astype(BF16)
        start(("zh", 2), zh.at[2], zr.at[2], to_z[2])

    def first_to_x():
        wait(("zh", 0), zr.at[0])
        wait(("zh", 2), zr.at[2])
        total = dd32[0, z] + zr[0].astype(F32) + zr[2].astype(F32)
        hx[0] = total.astype(BF16)
        start(("hx",), hx.at[0], hx.at[1], to_x)

    def first_to_y():
        wait(("hx",), hx.at[1])
        total = (hx[0].astype(F32) + hx[1].astype(F32)).astype(BF16)
        zr[0] = total
        hy[0] = zr[0, 1 - y]
        start(("hy",), hy.at[0], hy.at[1], to_y)
        for side in range(2):
            put(0, side, y, zr[0, y, side])

    def first_final():
        wait(("hy",), hy.at[1])
        for side in range(2):
            put(0, side, 1 - y, hy[1, side])

    def down_to_x(u, ks=(3, 2, 1, 0)):
        for k in ks:
            zd = z if k == 0 else z_of[k]
            start(("rx", u, k), ddb.at[u - 1, zd], rx.at[u - 1, zd], to_x)

    def down_along_z(u, k):
        zd = z if k == 0 else z_of[k]
        wait(("rx", u, k), rx.at[u - 1, zd])
        total = dd32[u, zd, :, rep] + rx[u - 1, zd].astype(F32)
        if k == 0:
            fin[u - 1] = total
            return
        if k == 2:
            wait(("rz", u, 3), rz.at[u - 1, 3])
            total = total + rz[u - 1, 3].astype(F32)
        zs[u - 1, k] = total.astype(BF16)
        start(("rz", u, k), zs.at[u - 1, k], rz.at[u - 1, k], to_z[2 if k == 2 else 1])

    def down_final(u):
        total = fin[u - 1]
        wait(("rz", u, 1), rz.at[u - 1, pl.ds(1, 2)])
        for k in (1, 2):
            total = total + rz[u - 1, k].astype(F32)
        zs[u - 1, 0] = total.astype(BF16)
        start(("ry", u), zs.at[u - 1, 0, 1 - y], ry.at[u - 1], to_y)
        if u == CHUNKS - 1:
            start(("fx", u, 1), zs.at[u - 1, 0, 1 - y], fx.at[u - 1, 1], to_xy)
        start(("fx", u, 0), zs.at[u - 1, 0, y], fx.at[u - 1, 0], to_x)
        put(u, rep, y, zs[u - 1, 0, y])

    def down_y(u):
        wait(("ry", u), ry.at[u - 1])
        if u < CHUNKS - 1:
            start(("fx", u, 1), ry.at[u - 1], fx.at[u - 1, 1], to_x)
        put(u, rep, 1 - y, ry[u - 1])

    def down_x(u):
        wait(("fx", u), fx.at[u - 1])
        put(u, 1 - rep, y, fx[u - 1, 0])
        put(u, 1 - rep, 1 - y, fx[u - 1, 1])

    n_cols = 512

    def back(first, chunks, add=False):
        def body(j, _):
            c = pl.ds(pl.multiple_of(j * n_cols, n_cols), n_cols)
            total = dn[pl.ds(first, half), c] if add else None
            for u in chunks:
                term = lax.dot_general(
                    dgu[u, pl.ds(first, half), :], wgu[u, c, :], over_cols,
                    preferred_element_type=F32,
                )
                total = term if total is None else total + term
            dn[pl.ds(first, half), c] = total
            return 0

        lax.fori_loop(0, width // n_cols, body, 0)

    def back_to_core(h, first):
        r = pl.ds(pl.multiple_of(first + (1 - tp) * half, half), half)
        sd[h] = dn[r, :].astype(BF16)
        start(("cd", h), sd.at[h], rd.at[h], to_c)

    def half_of(first, who):
        return pl.multiple_of(first + who * half, half)

    bpart = half // BACK_PARTS

    def back_to_y(i):
        if i == 0:
            wait(("cd", 0), rd.at[0])
        r = pl.ds(pl.multiple_of(other_tokens + tp * half + i * bpart, bpart), bpart)
        q = pl.ds(i * bpart, bpart)
        mine = dn[r, :].astype(BF16).astype(F32)
        sy[q, :] = (mine + rd[0, q, :].astype(F32)).astype(BF16)
        start(("yd", i), sy.at[q], yd.at[q], to_y)

    def gain_terms(first):
        def body(i, acc):
            r = pl.ds(pl.multiple_of(first + i * norm_rows, norm_rows), norm_rows)
            terms = dn[r, :] * (xall[r, :].astype(F32) * inv[r, :])
            return acc + jnp.sum(terms.reshape(norm_rows // 8, 8, width), axis=0)

        return lax.fori_loop(0, rows // norm_rows, body, jnp.zeros((8, width), F32))

    in_plane = rep * N_Y + y

    def gain_core():
        acc = gain_terms(own_tokens) + gain_terms(other_tokens)
        gvec[0] = jnp.sum(acc, axis=0, keepdims=True)
        start(("gc",), gvec.at[0], gvec.at[1], to_c)

    def gain_plane():
        wait(("gc",), gvec.at[1])
        gp[in_plane] = gvec[0] + gvec[1]
        here = gp.at[in_plane]
        for i, target in enumerate((to_y, to_x, to_xy)):
            start(("gp", i), here, here, target)

    def gain_z():
        wait(("gp",), gp.at[pl.ds(0, 3)])
        gz[z] = gp[0] + gp[1] + gp[2] + gp[3]
        for i in range(3):
            start(("gz", i), gz.at[z], gz.at[z], to_z[i + 1])

    def gain_end():
        wait(("gz",), gz.at[pl.ds(0, 3)])
        gg[...] = gz[0] + gz[1] + gz[2] + gz[3]

    out_row = pl.multiple_of(tp * half, half)

    def back_final(i):
        q = pl.ds(i * bpart, bpart)
        wait(("yd", i), yd.at[q])
        r = pl.ds(pl.multiple_of(own_tokens + tp * half + i * bpart, bpart), bpart)
        mine = dn[r, :].astype(BF16).astype(F32) + rd[1, q, :].astype(F32)
        mine = mine.astype(BF16).astype(F32) + yd[q, :].astype(F32)
        mine = mine.astype(BF16).astype(F32)
        scale = inv[r, :]
        unit = xall[r, :].astype(F32) * scale
        scaled = gain_row * mine
        mean = jnp.mean(scaled * unit, axis=-1, keepdims=True)
        o = pl.ds(pl.multiple_of(out_row + i * bpart, bpart), bpart)
        ig[o, :] = (ctall[r, :].astype(F32) + scale * (scaled - unit * mean)).astype(BF16)
        start(("ig", i), ig.at[o], ig.at[o], to_c)

    def gather_sent():
        sent("yw", span(3 * CHUNKS + 2 * TOKEN_PARTS * 2 * 2))
        sent("xw", span(3 * CHUNKS * (N_Z - 1)))
        for i in range(N_Z - 1):

            @pl.when(z == i)
            def _():
                sent("up", span(3 * CHUNKS * (i + 1)))

            @pl.when(z == N_Z - 1 - i)
            def _():
                sent("dn", span(3 * CHUNKS * (i + 1)))

    def y_upto(limit):
        def step(r):
            spent = 0
            for item in Y_ORDER[r]:
                cost = 1 if item[0] == "w" else 2
                if y_done[0] <= spent < limit:
                    y_step(r, item)
                spent += cost

        each_rep(step)
        y_done[0] = limit

    def core_token_group(a, parts):
        for i in parts:
            core_tokens(a, i)

    def tokens_ready(a):
        wait(("ct", a), (xall, ctall)[a].at[pl.ds(0, half)])

    y_done = [0]
    y_upto(1)
    for n in (0, 1, 2, 3):
        kept[n].start()
    kept_tokens[0].start()
    for n in range(4, len(pieces)):
        kept[n].start()
    kept_tokens[1].start()
    for n in (0, 1):
        kept[n].wait()
    own_send(0)
    kept_tokens[0].wait()
    y_upto(4)
    normalize(own_tokens)
    for copy in kept[2:] + kept_tokens[1:]:
        copy.wait()
    own_send(1)
    last = len(pieces)
    for t in range(last + 2):
        y_upto(3 * t + 7)
        if t + 2 < last and t + 2 >= 3:
            own_send(t + 2)
        for d in range(1, N_Z):
            if t == 8 and d == 3:
                tokens_ready(1)
                forward(0, other_tokens)
            if t == 9 and d == 3:
                first_to_z()
                chunk_ready(1)
                forward(1, own_tokens)
            if 0 <= t + 1 - d < last:
                arrive(t + 1 - d, d)
            if t == 0 and d == 1:
                own_send(2)
        if t == 2:
            core_token_group(0, (0, 1))
        if t == 4:
            core_token_group(0, (2, 3))
        if t == 5:
            tokens_ready(0)
            normalize(other_tokens)
        if t == 6:
            core_token_group(1, (0, 1))
            chunk_ready(0)
            forward(0, own_tokens)
        if t == 7:
            core_token_group(1, (2, 3))
        if t == 8:
            down_terms(0)
    forward(1, other_tokens)
    down_terms(1)
    down_to_x(1)
    early = tuple(range(CHUNKS - 1))
    final = CHUNKS - 1
    back(half_of(other_tokens, 1 - tp), early)
    back(half_of(other_tokens, tp), early)
    chunk_ready(final)
    forward(final, other_tokens)
    back(half_of(other_tokens, 1 - tp), (final,), True)
    back_to_core(0, other_tokens)
    first_on_z()
    down_along_z(1, 3)
    back(half_of(other_tokens, tp), (final,), True)
    for i in range(BACK_PARTS - 2):
        back_to_y(i)
    forward(2, own_tokens)
    down_along_z(1, 1)
    down_terms(2)
    down_to_x(2)
    back(half_of(own_tokens, 1 - tp), range(CHUNKS))
    back_to_core(1, own_tokens)
    down_along_z(1, 2)
    down_along_z(1, 0)
    back(half_of(own_tokens, tp), range(CHUNKS))
    down_along_z(2, 3)
    gain_core()
    gain_plane()
    for i in range(BACK_PARTS - 2, BACK_PARTS):
        back_to_y(i)
    first_to_x()
    wait(("cd", 1), rd.at[1])
    down_along_z(2, 2)
    down_along_z(2, 1)
    down_final(1)
    back_final(0)
    back_final(1)
    down_along_z(2, 0)
    gather_sent()
    gain_z()
    back_final(2)
    back_final(3)
    back_final(4)
    back_final(5)
    first_to_y()
    down_final(2)
    down_y(1)
    back_final(6)
    back_final(7)
    down_x(1)
    gain_end()
    first_final()
    down_y(2)
    down_x(2)
    wait(("ig",), ig.at[pl.ds(0, half)])
    rest = (CHUNKS - 1) * (N_Z + N_Z - 1) + 3 * (CHUNKS - 1) // 2 + 3 * 2 + 2 + 1
    moved = 2 * half * width // (wrows * uc)
    sent("late", span(rest + 2 * moved))
    sent("gc", gp.at[pl.ds(0, 7)])

def fused(x, gain, gate_w, up_w, down_w, ct):
    rows, width = x.shape
    wrows, cols = gate_w.shape
    units = cols // N_Y
    uc = units // CHUNKS
    half = rows // 2
    n = len(all_slots())
    vm = pltpu.VMEM
    anywhere = pl.BlockSpec(memory_space=pl.ANY)
    tile = (2, wrows // 2, uc)
    ig, gg, dd = pl.pallas_call(
        fused_kernel,
        out_shape=[
            vm((rows, width), BF16),
            vm((1, width), F32),
            vm((wrows, cols), F32),
        ],
        in_specs=[anywhere, pl.BlockSpec(memory_space=vm)] + [anywhere] * 4,
        out_specs=[pl.BlockSpec(memory_space=vm)] * 3,
        scratch_shapes=[
            vm((CHUNKS, width, 2 * uc), BF16),
            vm((CHUNKS, width, uc), BF16),
            vm((2 * rows, width), BF16),
            vm((2 * rows, width), BF16),
            vm((2 * rows, width), BF16),
            vm((2 * rows, 1), F32),
            vm((CHUNKS, 2 * rows, uc), BF16),
            vm((CHUNKS, 2 * rows, 2 * uc), BF16),
            vm((2 * rows, width), F32),
            vm((CHUNKS, N_Z, 2) + tile, F32),
            vm((CHUNKS - 1, N_Z) + tile, BF16),
            vm((CHUNKS - 1, N_Z) + tile, BF16),
            vm((CHUNKS - 1, N_Z) + tile, BF16),
            vm((CHUNKS - 1, N_Z) + tile, BF16),
            vm((CHUNKS - 1,) + tile, F32),
            vm((CHUNKS - 1,) + tile[1:], BF16),
            vm((CHUNKS - 1,) + tile, BF16),
            vm((2, half, width), BF16),
            vm((2, half, width), BF16),
            vm((half, width), BF16),
            vm((half, width), BF16),
            vm((8, 1, width), F32),
            vm((N_Z, 1, width), F32),
            vm((2, 1, width), F32),
            vm((3, 2) + tile, BF16),
            vm((3, 2) + tile, BF16),
            vm((2, 2) + tile, BF16),
            vm((2,) + tile, BF16),
            pltpu.SemaphoreType.DMA((LATE + 1,)),
            pltpu.SemaphoreType.DMA((n,)),
            pltpu.SemaphoreType.DMA((2 + 3 * CHUNKS,)),
        ],
        compiler_params=pltpu.CompilerParams(
            collective_id=0, has_side_effects=True, vmem_limit_bytes=62500000
        ),
        name="fused",
    )(x, gain.reshape(1, width), gate_w, up_w, down_w, ct)
    return ig, gg.reshape(width), dd


def shift(value, axis, step):
    size = lax.axis_size(axis)
    return lax.ppermute(value, axis, [(i, (i + step) % size) for i in range(size)])


def swap(value, axis, bit):
    return lax.ppermute(value, axis, [(i, i ^ bit) for i in range(lax.axis_size(axis))])


def summed_everywhere(value):
    for axis in ("rep", "fs", "tp"):
        size = lax.axis_size(axis)
        if size & (size - 1):
            value = lax.psum(value, axis)
            continue
        bit = 1
        while bit < size:
            value = value + swap(value, axis, bit)
            bit *= 2
    return value


def local(inputs, gain, gate_weight, up_weight, down_weight, cotangent):
    n_rep, n_tp = lax.axis_size("rep"), lax.axis_size("tp")
    if (n_rep, lax.axis_size("fs"), n_tp) == (2, N_Y * N_Z, 2):
        return fused(inputs, gain, gate_weight, up_weight, down_weight, cotangent)
    rep, tp = lax.axis_index("rep"), lax.axis_index("tp")
    rows, width = inputs.shape
    block = rows // n_tp
    units = gate_weight.shape[1] // n_rep

    def own_units(weight):
        return lax.dynamic_slice_in_dim(weight, rep * units, units, axis=1)

    def own_block(value, step):
        return lax.dynamic_slice_in_dim(value, (tp + step) % n_tp * block, block, axis=0)

    def gathered_tokens(value):
        parts = [own_block(value, s) for s in range(n_tp)]
        for j in range(1, n_rep):
            first = shift(own_block(value, 0), "rep", -j)
            parts += [first] + [shift(first, "tp", -s) for s in range(1, n_tp)]
        return jnp.concatenate(parts, axis=0)

    both_own = jnp.concatenate([own_units(gate_weight), own_units(up_weight)], axis=1)
    both_full = lax.all_gather(both_own, "fs", axis=0, tiled=True)
    down_full = lax.all_gather(own_units(down_weight), "fs", axis=0, tiled=True)
    tokens = gathered_tokens(inputs)
    cots = gathered_tokens(cotangent)

    def normed(value):
        single = value.astype(jnp.float32)
        inv = lax.rsqrt(jnp.mean(single * single, axis=-1, keepdims=True) + EPS)
        return single * inv, inv

    normalized_input = (normed(tokens)[0] * gain).astype(jnp.bfloat16)
    contract_cols = (((1,), (1,)), ((), ()))
    contract_rows = (((0,), (0,)), ((), ()))
    both = jnp.dot(normalized_input, both_full, preferred_element_type=jnp.float32)
    gate, up_proj = both[:, :units], both[:, units:]
    gate_sig = jax.nn.sigmoid(gate)
    active = gate * gate_sig
    hidden = (active * up_proj).astype(jnp.bfloat16)
    d_down_terms = (
        0.5 * lax.dot_general(cots, hidden, contract_rows, preferred_element_type=jnp.float32)
    ).astype(jnp.bfloat16)
    d_down_terms, cots = lax.optimization_barrier((d_down_terms, cots))
    summed = lax.psum_scatter(d_down_terms, "fs", scatter_dimension=0, tiled=True)
    d_hidden = 0.5 * jnp.dot(cots, down_full, preferred_element_type=jnp.float32)
    d_gate = (d_hidden * up_proj * gate_sig * (1.0 + gate * (1.0 - gate_sig))).astype(jnp.bfloat16)
    d_up = (d_hidden * active).astype(jnp.bfloat16)
    partial_value = (
        lax.dot_general(
            jnp.concatenate([d_gate, d_up], axis=1),
            both_full,
            contract_cols,
            preferred_element_type=jnp.float32,
        )
    ).astype(jnp.bfloat16).reshape(n_rep, n_tp, block, width)

    def tp_terms(step):
        return partial_value[:, step]

    over_tp = tp_terms(0).astype(jnp.float32)
    for s in range(1, n_tp):
        over_tp = over_tp + shift(tp_terms(s), "tp", s).astype(jnp.float32)
    over_tp = over_tp.astype(jnp.bfloat16)
    total = over_tp[0].astype(jnp.float32)
    for j in range(1, n_rep):
        total = total + shift(over_tp[j], "rep", j).astype(jnp.float32)
    normalized_gradient = total.astype(jnp.bfloat16).astype(jnp.float32)
    unit_input, inv = normed(own_block(inputs, 0))
    gain_gradient = summed_everywhere(jnp.sum(normalized_gradient * unit_input, axis=0))
    gain_scaled = gain * normalized_gradient
    mean_correction = jnp.mean(gain_scaled * unit_input, axis=-1, keepdims=True)
    block_gradient = (
        own_block(cotangent, 0).astype(jnp.float32)
        + inv * (gain_scaled - unit_input * mean_correction)
    ).astype(jnp.bfloat16)
    input_gradient = jnp.zeros((rows, width), jnp.bfloat16)
    for s in range(n_tp):
        piece = block_gradient if s == 0 else shift(block_gradient, "tp", -s)
        input_gradient = lax.dynamic_update_slice_in_dim(
            input_gradient, piece, (tp + s) % n_tp * block, axis=0
        )
    d_down = jnp.zeros((summed.shape[0], units * n_rep), jnp.float32)
    for j in range(n_rep):
        piece = summed if j == 0 else shift(summed, "rep", -j)
        d_down = lax.dynamic_update_slice_in_dim(
            d_down, piece.astype(jnp.float32), (rep + j) % n_rep * units, axis=1
        )
    return (input_gradient, gain_gradient, d_down)


def solution(mesh):
    placed = (
        P(("rep", "fs"), None),
        P(),
        P("fs", "tp"),
        P("fs", "tp"),
        P("fs", "tp"),
        P(("rep", "fs"), None),
    )
    return jax.shard_map(
        local,
        mesh=mesh,
        in_specs=placed,
        out_specs=(P(("rep", "fs"), None), P(), P("fs", "tp")),
        check_vma=False,
    )
```
